256 devices in a mesh: kv: 32 (over z, x), tp: 8 (over y, core).
Axes of the slice: x: 4, y: 4, z: 8, core: 2. Of those that a mesh axis runs over, the one named last changes fastest.
Arguments:
- tokens: bfloat16 [18, 4096], P(None, ('kv', 'tp')), may hold values from -12.2 to 12.2
- norm_gains: float32 [6, 4096], replicated, may hold values from 0.1 to 1.9
- first_gate: bfloat16 [4096, 11264], P(None, ('kv', 'tp')), may hold values from -0.09375 to 0.09375
- first_lift: bfloat16 [4096, 11264], P(None, ('kv', 'tp')), may hold values from -0.09375 to 0.09375
- first_down: bfloat16 [11264, 4096], P(('kv', 'tp')), may hold values from -0.25 to 0.25
- query_weight: bfloat16 [4096, 4096], P('kv', 'tp'), may hold values from -0.09375 to 0.09375
- key_weight: bfloat16 [4096, 4096], P('kv', 'tp'), may hold values from -0.09375 to 0.09375
- value_weight: bfloat16 [4096, 4096], P('kv', 'tp'), may hold values from -0.09375 to 0.09375
- forget_weight: bfloat16 [4096, 64], P(None, 'tp'), may hold values from -0.25 to 0.25
- output_weight: bfloat16 [4096, 4096], P('tp', 'kv'), may hold values from -0.09375 to 0.09375
- second_gate: bfloat16 [4096, 11264], P(None, ('kv', 'tp')), may hold values from -0.09375 to 0.09375
- second_lift: bfloat16 [4096, 11264], P(None, ('kv', 'tp')), may hold values from -0.09375 to 0.09375
- second_down: bfloat16 [11264, 4096], P(('kv', 'tp')), may hold values from -0.25 to 0.25
- cache_keys: bfloat16 [18, 8192, 4096], P(None, 'kv', 'tp'), may hold values from -457 to 457
- cache_values: bfloat16 [18, 8192, 4096], P(None, 'kv', 'tp'), may hold values from -6 to 6
- cache_decay: float32 [18, 64, 8192], P(None, 'tp', 'kv'), may hold values from -2500 to 0, as said below
Outputs:
- layer_out: bfloat16 [18, 4096], P(None, ('kv', 'tp'))
The draws below stay inside these ranges and needn't reach their ends.
Inputs may be any that keep to these rules, and one draw needn't show every extreme that they name: `cache_decay`: each entry is a sum of log forget gates, each at most zero, of the later cached positions of the same sequence and head, so entries never fall along positions and the last is zero.
All inputs are finite; a program needn't handle non-finite values.
Results may differ from the reference program's by a relative error of at most 0.025.
Values may be sent and summed in bfloat16 or wider, within the bound.
A program may use at most 64 MiB of HBM per device.

```python
import math
import jax
import jax.numpy as jnp
from jax import lax

D = 4096
HEADS = 64
HD = 64
FF = 11264
SEQUENCE_COUNT = 18
POS_DEV = 256
CACHED_POSITIONS = 8192
KW = 4096
N_KV = 32
N_TP = 8


def draw_tokens(key, part):
    first_key, second_key = jax.random.split(key)
    column_ramp = jnp.arange(D, dtype=jnp.float32) / (D - 1) - 0.5
    sample = jnp.clip(jax.random.normal(first_key, (SEQUENCE_COUNT, D), jnp.float32), -5.0, 5.0)
    column_scale = 3.0 ** column_ramp
    roughness = jax.random.uniform(second_key, (1, D), jnp.float32, 0.6, 1.4)
    return (sample * column_scale[None, :] * roughness).astype(jnp.bfloat16)


def draw_cache_keys(key, part):
    random_key_split = jax.random.split(key, 1)
    sample = jnp.clip(jax.random.normal(random_key_split[0], (SEQUENCE_COUNT, CACHED_POSITIONS, KW), jnp.float32), -5.0, 5.0)
    return sample.astype(jnp.bfloat16)


def draw_cache_decay(key, part):
    random_key_split = jax.random.split(key, 7)
    full_shape = (SEQUENCE_COUNT, HEADS, CACHED_POSITIONS)
    slow_share = 0.5
    slow_heads = jax.random.uniform(random_key_split[0], (SEQUENCE_COUNT, HEADS, 1), jnp.float32) < slow_share
    slow_total = jax.random.uniform(random_key_split[1], (SEQUENCE_COUNT, HEADS, 1), jnp.float32, 0.3, 0.8)
    fast_rate = jnp.exp(jax.random.uniform(random_key_split[2], (SEQUENCE_COUNT, HEADS, 1), jnp.float32, math.log(0.03), math.log(0.1)))
    baseline_rate = jnp.where(slow_heads, slow_total / CACHED_POSITIONS, fast_rate)
    block_count = CACHED_POSITIONS // POS_DEV
    block_multiplier = jnp.exp(jax.random.uniform(random_key_split[3], (SEQUENCE_COUNT, HEADS, block_count, 1), jnp.float32, math.log(0.5), math.log(1.5)))
    block_multiplier = jnp.broadcast_to(block_multiplier, (SEQUENCE_COUNT, HEADS, block_count, POS_DEV)).reshape(full_shape)
    random_noise = jax.random.uniform(random_key_split[4], full_shape, jnp.float32, 0.2, 1.8)
    spike_position = jax.random.randint(random_key_split[5], (SEQUENCE_COUNT, 2), 0, CACHED_POSITIONS)
    spike_penalty = jax.random.uniform(random_key_split[6], (SEQUENCE_COUNT, 2), jnp.float32, 0.2, 0.4)
    position_index = jnp.arange(CACHED_POSITIONS)
    sudden_spike = jnp.sum(jnp.where(position_index[None, None, :] == spike_position[:, :, None], jnp.log(1.0 - spike_penalty)[:, :, None], 0.0), axis=1)
    gate_values = -baseline_rate * block_multiplier * random_noise + sudden_spike[:, None, :]
    running = jnp.cumsum(gate_values, axis=2)
    return running[:, :, -1:] - running


def spiked(entries, own_key, source, target, parts, factor):
    owner, partner = [(jnp.arange(entries.shape[axis_at]) // (entries.shape[axis_at] // parts)).reshape([-1 if axis == axis_at else 1 for axis in range(entries.ndim)]) for axis_at in (source, target)]
    chosen = jax.random.permutation(own_key, parts)[partner]
    strong = (owner == chosen) | (owner == (partner + parts // 2) % parts)
    return jnp.where(strong, factor * entries, entries)


def block_scale(key, dims, shards, smallest, top_value):
    factor_of, own = 1.0, jax.random.fold_in(key, 6)
    for axis_at, blocks in shards:
        heights = jnp.exp(jax.random.uniform(jax.random.fold_in(own, axis_at), (blocks,), jnp.float32, smallest / len(shards), top_value / len(shards)))
        factor_of = factor_of * jnp.repeat(heights, dims[axis_at] // blocks).reshape([-1 if axis == axis_at else 1 for axis in range(len(dims))])
    return factor_of


def centred(key, dims, deviation, bound, shards=(), held_as=jnp.bfloat16):
    loudness = block_scale(key, dims, shards, -0.22, 0.18) if shards else 1.0
    drawn = jax.random.normal(key, dims, jnp.float32) * deviation * loudness
    return jnp.minimum(jnp.maximum(drawn, -bound), bound).astype(held_as)


def gaussian_with(rng, shape, width, limit, pieces, heavy, kind=jnp.bfloat16):
    entries = width * jax.random.normal(rng, shape, jnp.float32)
    if pieces:
        entries = entries * block_scale(rng, shape, pieces, -0.22, 0.18)
    return jnp.clip(spiked(entries, jax.random.fold_in(rng, 3), *heavy), -limit, limit).astype(kind)


def setup_inputs(seed: int = 0) -> dict:
    streams_of = jax.random.split(jax.random.key(seed), 17)
    return {
        "tokens": draw_tokens(jax.random.fold_in(streams_of[16], 71), 0),
        "norm_gains": jnp.clip(1.0 + 0.18 * jax.random.normal(streams_of[1], (6, D), jnp.float32), 0.1, 1.9),
        "first_gate": centred(streams_of[2], (D, FF), D ** -0.5, 0.09375, ((1, 256),)),
        "first_lift": centred(streams_of[3], (D, FF), D ** -0.5, 0.09375, ((1, 256),)),
        "first_down": gaussian_with(streams_of[4], (FF, D), FF ** -0.5, 0.25, ((0, 256),), (0, 1, 256, 6.0)),
        "query_weight": centred(streams_of[5], (D, KW), D ** -0.5, 0.09375, ((0, 32), (1, 8))),
        "key_weight": centred(streams_of[6], (D, KW), D ** -0.5, 0.09375, ((0, 32), (1, 8))),
        "value_weight": centred(streams_of[7], (D, KW), D ** -0.5, 0.09375, ((0, 32), (1, 8))),
        "forget_weight": centred(streams_of[8], (D, HEADS), (D // 9) ** -0.5, 0.25, ((1, 8),)),
        "output_weight": centred(streams_of[9], (KW, D), KW ** -0.5, 0.09375, ((0, 8), (1, 32))),
        "second_gate": centred(streams_of[10], (D, FF), D ** -0.5, 0.09375, ((1, 256),)),
        "second_lift": centred(streams_of[11], (D, FF), D ** -0.5, 0.09375, ((1, 256),)),
        "second_down": gaussian_with(streams_of[12], (FF, D), FF ** -0.5, 0.25, ((0, 256),), (0, 1, 256, 6.0)),
        "cache_keys": draw_cache_keys(jax.random.fold_in(streams_of[16], 71), 0),
        "cache_values": centred(streams_of[14], (SEQUENCE_COUNT, CACHED_POSITIONS, KW), 1.0, 6.0, ((1, 32), (2, 8))),
        "cache_decay": draw_cache_decay(jax.random.fold_in(streams_of[16], 71), 0),
    }


epsilon = 1e-06

def root_norm(values, norm_gain):
    return values * lax.rsqrt(lax.optimization_barrier(jnp.mean(values * values, axis=-1, keepdims=True)) + epsilon) * norm_gain

def settle(values):
    return lax.optimization_barrier(values.astype(jnp.bfloat16)).astype(jnp.float32)

def gated_half(stream, pre_gain, post_gain, gate_matrix, lift_matrix, down_matrix):
    normed = root_norm(stream, pre_gain).astype(jnp.bfloat16)
    gate_part = jnp.dot(normed, gate_matrix, preferred_element_type=jnp.float32)
    lift_part = jnp.dot(normed, lift_matrix, preferred_element_type=jnp.float32)
    active = (jax.nn.silu(gate_part) * lift_part).astype(jnp.bfloat16)
    branch = settle(jnp.dot(active, down_matrix, preferred_element_type=jnp.float32))
    return stream + 0.5 * root_norm(branch, post_gain)

def attend_one(inputs):
    queries, key_new, value_new, forget, key_rows, value_rows, decay_rows = inputs
    score_scale = HD ** (-0.5)
    query_heads = queries.reshape(HEADS, HD).astype(jnp.float32)
    key_heads = key_rows.reshape(N_KV, POS_DEV, HEADS, HD).astype(jnp.float32)
    value_heads = value_rows.reshape(N_KV, POS_DEV, HEADS, HD).astype(jnp.float32)
    scores = jnp.einsum('hd,nphd->hnp', query_heads, key_heads) * score_scale
    scores = scores + forget[:, None, None] + decay_rows.reshape(HEADS, N_KV, POS_DEV)
    block_peak = lax.optimization_barrier(jnp.max(scores, axis=2))
    raised = jnp.exp(scores - block_peak[:, :, None])
    totals = lax.optimization_barrier(jnp.sum(raised, axis=2))
    weights = settle(raised)
    block_out = settle(jnp.einsum('hnp,nphd->hnd', weights, value_heads) / totals[:, :, None])
    own_score = lax.optimization_barrier(jnp.sum(query_heads * key_new.reshape(HEADS, HD).astype(jnp.float32), axis=1)) * score_scale
    summit = jnp.maximum(own_score, lax.optimization_barrier(jnp.max(block_peak, axis=1)))
    block_weight = totals * jnp.exp(block_peak - summit[:, None])
    own_weight = jnp.exp(own_score - summit)
    summed = lax.optimization_barrier(jnp.sum(block_weight[:, :, None] * block_out, axis=1))
    summed = summed + own_weight[:, None] * value_new.reshape(HEADS, HD).astype(jnp.float32)
    joined = summed / (lax.optimization_barrier(jnp.sum(block_weight, axis=1)) + own_weight)[:, None]
    return joined.astype(jnp.bfloat16).reshape(HEADS * HD)

def reference(tokens, norm_gains, first_gate, first_lift, first_down, query_weight, key_weight, value_weight, forget_weight, output_weight, second_gate, second_lift, second_down, cache_keys, cache_values, cache_decay):
    stream = tokens.astype(jnp.float32)
    middle = gated_half(stream, norm_gains[0], norm_gains[1], first_gate, first_lift, first_down)
    normed = root_norm(middle, norm_gains[2]).astype(jnp.bfloat16)
    queries = jnp.dot(normed, query_weight, preferred_element_type=jnp.float32).astype(jnp.bfloat16)
    key_new = jnp.dot(normed, key_weight, preferred_element_type=jnp.float32).astype(jnp.bfloat16)
    value_new = jnp.dot(normed, value_weight, preferred_element_type=jnp.float32).astype(jnp.bfloat16)
    forget = jax.nn.log_sigmoid(jnp.dot(normed, forget_weight, preferred_element_type=jnp.float32))
    attended = lax.map(attend_one, (queries, key_new, value_new, forget, cache_keys, cache_values, cache_decay))
    seq_count = tokens.shape[0]
    head_groups = attended.reshape(seq_count, N_TP, KW // N_TP).astype(jnp.float32)
    weight_groups = output_weight.reshape(N_TP, KW // N_TP, D).astype(jnp.float32)
    partials = settle(jnp.einsum('bnk,nkd->bnd', head_groups, weight_groups))
    mixed_rows = settle(lax.optimization_barrier(jnp.sum(partials, axis=1)))
    after_mix = middle + root_norm(mixed_rows, norm_gains[3])
    layer_out = gated_half(after_mix, norm_gains[4], norm_gains[5], second_gate, second_lift, second_down)
    return layer_out.astype(jnp.bfloat16)
```

```python
import functools

import jax
import jax.numpy as jnp
from jax import lax
from jax.experimental import pallas as pl
from jax.experimental.pallas import tpu as pltpu
from jax.sharding import PartitionSpec as P

MESH = pl.DeviceIdType.MESH
F32, BF16 = jnp.float32, jnp.bfloat16
EPS = 1e-06
HD = 64
LANES = 128
NX = 4
STAGES = 15
(T_TOK, K_TOK, R_TOKQ, R_F1, T_F1, R_QKV, K_B, K_Q, R_ATT, K_ATT, T_MIX, K_MIX, R_F2, T_F2, K_STAT) = range(STAGES)


def nt(a, b):
    return lax.dot_general(a, b, (((1,), (1,)), ((), ())), preferred_element_type=F32)


def nn(a, b):
    return jnp.dot(a, b, preferred_element_type=F32)


def lane_sum(v):
    return jnp.sum(v, axis=-1, keepdims=True)


def silu(v):
    return v / (1.0 + jnp.exp(-v))


def kernel(
    n_kv, n_tp, seqs, width,
    tok_h, gains_h, g1_h, l1_h, d1_h, wq_h, wk_h, wv_h, wf_h, wo_h, g2_h, l2_h, d2_h, ck_h, cv_h, cd_h,
    out_ref,
    tok, gains, g1, l1, d1, wq, wk, wv, wf, wo, g2, l2, d2, ck, cv, cd,
    ttok, xb, xn, piece, sq1, rq1, pf, rf, tf, sqk, rqk, bb, qb, sat, rat, ab, tm, mb, mid, pf2, rf2, tf2, stb, kept,
    load_sem, ssem, rsem,
):
    kv, tp = lax.axis_index("kv"), lax.axis_index("tp")
    nz = n_kv // NX
    zz, xx = kv // NX, kv % NX
    col = pl.multiple_of(kv * LANES, LANES)
    heads = cd.shape[1]
    groups = heads * HD // LANES

    loads = [
        pltpu.make_async_copy(h, v, load_sem.at[i])
        for i, (h, v) in enumerate(
            [(tok_h, tok), (gains_h, gains), (wq_h, wq), (wk_h, wk), (wv_h, wv), (wf_h, wf), (g1_h, g1), (l1_h, l1),
             (d1_h, d1), (ck_h, ck), (cd_h, cd), (cv_h, cv), (wo_h, wo), (g2_h, g2), (l2_h, l2), (d2_h, d2)]
        )
    ]
    for copy in loads:
        copy.start()

    def owner_of(b):
        return (n_kv * b + seqs - 1) // seqs

    my_seq = (kv * seqs) // n_kv
    owns = owner_of(my_seq) == kv

    def kv_peer(i):
        a, c = i // NX, i % NX
        dz = (nz // 2 + ((a + 1) // 2) * (1 - 2 * (a % 2)) + nz) % nz
        dx = (NX // 2 + ((c + 1) // 2) * (1 - 2 * (c % 2)) + NX) % NX
        return ((zz + dz) % nz) * NX + (xx + dx) % NX

    def tp_peer(i):
        return (tp + 1 + i) % n_tp

    def send(src, dst, stage, **where):
        pltpu.make_async_remote_copy(
            src_ref=src, dst_ref=dst, send_sem=ssem.at[stage], recv_sem=rsem.at[stage],
            device_id=where, device_id_type=MESH,
        ).start()

    def wait(sem, ref):
        pltpu.make_async_copy(ref, ref, sem).wait()

    def to_all_kv(buf, slot, stage):
        @pl.loop(0, n_kv - 1)
        def _(i):
            send(buf.at[slot], buf.at[slot], stage, kv=kv_peer(i))

    def to_all_tp(buf, stage):
        @pl.loop(0, n_tp - 1)
        def _(i):
            send(buf.at[tp], buf.at[tp], stage, tp=tp_peer(i))

    def got_kv(buf, stage):
        wait(rsem.at[stage], buf.at[pl.ds(0, n_kv - 1)])

    def got_tp(buf, stage):
        wait(rsem.at[stage], buf.at[pl.ds(0, n_tp - 1)])

    def to_kv_blocks(src, dst, stage):
        @pl.loop(0, n_kv - 1)
        def _(i):
            k = kv_peer(i)
            send(src.at[k], dst.at[kv], stage, kv=k)

        dst[kv] = src[kv]

    def send_owner(src, dst, b, stage):
        @pl.when(owner_of(b) != kv)
        def _():
            send(src.at[b], dst.at[kv], stage, kv=owner_of(b))

    def to_owners(src, dst, stage):
        @pl.loop(0, seqs)
        def _(b):
            send_owner(src, dst, b, stage)

        @pl.when(owns)
        def _():
            dst[kv] = src[my_seq]

    def got_from_owners(buf, sem):
        @pl.when(owns)
        def _():
            wait(sem, buf.at[pl.ds(0, seqs - 1)])

        @pl.when(jnp.logical_not(owns))
        def _():
            wait(sem, buf.at[pl.ds(0, seqs)])

    barrier = pltpu.get_barrier_semaphore()

    @pl.loop(0, n_kv - 1)
    def _(i):
        pl.semaphore_signal(barrier, inc=1, device_id={"kv": kv_peer(i)}, device_id_type=MESH)

    @pl.loop(0, n_tp - 1)
    def _(i):
        pl.semaphore_signal(barrier, inc=1, device_id={"tp": tp_peer(i)}, device_id_type=MESH)

    loads[0].wait()
    own_w = tok.shape[0]
    lane = lax.broadcasted_iota(jnp.int32, (own_w, LANES), 1)
    row = lax.broadcasted_iota(jnp.int32, (own_w, LANES), 0)
    place = jnp.where(lane == row + own_w * tp, 1.0, 0.0).astype(BF16)
    ttok[tp] = lax.dot_general(tok[...], place, (((0,), (0,)), ((), ())), preferred_element_type=F32).astype(BF16)

    pl.semaphore_wait(barrier, n_kv + n_tp - 2)

    to_all_tp(ttok, T_TOK)
    got_tp(ttok, T_TOK)
    tblk = functools.reduce(lambda a, k: a + ttok[k].astype(F32), range(1, n_tp), ttok[0].astype(F32))
    xb[kv] = tblk.astype(BF16)
    to_all_kv(xb, kv, K_TOK)

    for i in range(1, 6):
        loads[i].wait()

    def gain(i, k=None):
        return gains[i : i + 1, pl.ds(col, LANES)] if k is None else gains[i : i + 1, k * LANES : (k + 1) * LANES]

    lane_s = lax.broadcasted_iota(jnp.int32, (seqs, LANES), 1)

    def projections(x, stats, out):
        parts = [nn(x, w[...]) for w in (wq, wk, wv)]
        for i, part in enumerate(parts):
            for j in range(groups):
                piece[:, i * groups + j, :] = part[:, j * LANES : (j + 1) * LANES]
        gates = nt(x, wf[:, pl.ds(col, LANES)])
        for j in range(groups):
            line = jnp.where(lane_s == 0, gates[:, 2 * j : 2 * j + 1], 0.0)
            line = line + jnp.where(lane_s == HD, gates[:, 2 * j + 1 : 2 * j + 2], 0.0)
            if j == 0:
                for n, stat in enumerate(stats):
                    high = stat.astype(BF16).astype(F32)
                    line = line + jnp.where(lane_s == n + 1, high, 0.0)
                    line = line + jnp.where(lane_s == HD + n + 1, stat - high, 0.0)
            piece[:, 3 * groups + j, :] = line
        out[...] = piece[...].astype(BF16)

    projections((tblk * gain(2)).astype(BF16), [lane_sum(tblk * tblk)], sq1)
    to_owners(sq1, rq1, R_TOKQ)

    def feed_forward(gate_w, lift_w, down_w, part_out):
        x = xn[...]
        act = (silu(nt(x, gate_w[...])) * nt(x, lift_w[...])).astype(BF16)
        for c in range(0, n_kv, 4):
            part = nn(act, down_w[:, c * LANES : (c + 4) * LANES])
            for j in range(4):
                part_out[c + j] = part[:, j * LANES : (j + 1) * LANES].astype(BF16)

    def block_sum(buf):
        total = buf[0].astype(F32)
        for k in range(1, n_kv):
            total = total + buf[k].astype(F32)
        return total

    def tp_sum(buf):
        return functools.reduce(lambda a, k: a + buf[k].astype(F32), range(1, n_tp), buf[0].astype(F32))

    got_kv(xb, K_TOK)
    squares = jnp.zeros((seqs, LANES), F32)
    for k in range(n_kv):
        v = xb[k].astype(F32)
        squares = squares + v * v
    scale = lax.rsqrt(lane_sum(squares) / width + EPS)
    for k in range(n_kv):
        xn[:, k * LANES : (k + 1) * LANES] = (xb[k].astype(F32) * scale * gain(0, k)).astype(BF16)
    for i in range(6, 9):
        loads[i].wait()
    feed_forward(g1, l1, d1, pf)
    to_kv_blocks(pf, rf, R_F1)
    got_kv(rf, R_F1)
    tf[tp] = block_sum(rf).astype(BF16)
    to_all_tp(tf, T_F1)
    got_tp(tf, T_F1)
    bblk = tp_sum(tf).astype(BF16)
    bb[kv] = bblk
    bf = bblk.astype(F32)
    u = bf * gain(1)
    projections((u * gain(2)).astype(BF16), [lane_sum(bf * bf), lane_sum(tblk * u), lane_sum(u * u)], sqk)
    to_owners(sqk, rqk, R_QKV)
    to_all_kv(bb, kv, K_B)

    low = lax.broadcasted_iota(jnp.int32, (groups, LANES), 1) < HD

    def halves(a, b):
        return jnp.where(low, a, b)

    lane_1 = lax.broadcasted_iota(jnp.int32, (1, LANES), 1)

    def stat_of(line, n):
        return lane_sum(jnp.where((lane_1 == n + 1) | (lane_1 == HD + n + 1), line, 0.0))

    def own_rows():
        asum, bsum = block_sum(rq1), block_sum(rqk)
        at, bt = 3 * groups, 3 * groups + 1
        s_b, s_tu, s_uu = [stat_of(bsum[at:bt], n) for n in range(3)]
        r1 = lax.rsqrt(s_b / width + EPS)
        s_mid = stat_of(asum[at:bt], 0) + r1 * s_tu + 0.25 * r1 * r1 * s_uu
        scale_mid = lax.rsqrt(s_mid / width + EPS)
        full = scale_mid * (asum + 0.5 * r1 * bsum)
        q, k, v, f = [full[i * groups : (i + 1) * groups] for i in range(4)]
        q, k, v = [t.astype(BF16).astype(F32) for t in (q, k, v)]
        f = halves(f[:, 0:1], f[:, HD : HD + 1])
        forget = jnp.minimum(f, 0.0) - jnp.log(1.0 + jnp.exp(-jnp.abs(f)))
        qk = q * k
        own = halves(lane_sum(jnp.where(low, qk, 0.0)), lane_sum(jnp.where(low, 0.0, qk))) * (HD**-0.5) - forget
        return q, own, v

    @pl.when(owns)
    def _():
        got_kv(rq1, R_TOKQ)
        got_kv(rqk, R_QKV)
        q, own, v = own_rows()
        qb[my_seq] = q
        kept[0] = own
        kept[1] = v
        to_all_kv(qb, my_seq, K_Q)

    got_from_owners(qb, rsem.at[K_Q])

    for i in range(9, 12):
        loads[i].wait()
    head_i = lax.broadcasted_iota(jnp.int32, (heads, LANES), 0)
    lane_h = lax.broadcasted_iota(jnp.int32, (heads, LANES), 1)
    masks = [head_i == 2 * j + lane_h // HD for j in range(groups)]

    @pl.loop(0, seqs)
    def _(b):
        rows = [jnp.where(masks[j], jnp.broadcast_to(qb[b, j : j + 1, :], (heads, LANES)), 0.0) for j in range(groups)]
        query = jnp.concatenate(rows, axis=1).astype(BF16)
        score = nt(query, ck[b]) * (HD**-0.5) + cd[b]
        peak = jnp.max(score, axis=1, keepdims=True)
        raised = jnp.exp(score - peak)
        total = lane_sum(raised)
        o = nn(raised.astype(BF16), cv[b]) / total
        level = jnp.broadcast_to(peak + jnp.log(total), (heads, LANES))
        for j in range(groups):
            oj = jnp.where(masks[j], o[:, j * LANES : (j + 1) * LANES], 0.0)
            sat[b, j : j + 1, :] = jnp.sum(oj, axis=0, keepdims=True)
            lj = jnp.where(masks[j], level, 0.0)
            sat[b, groups + j : groups + j + 1, :] = jnp.sum(lj, axis=0, keepdims=True)
        send_owner(sat, rat, b, R_ATT)

    @pl.when(owns)
    def _():
        rat[kv] = sat[my_seq]
        got_kv(rat, R_ATT)
        own_keep, v_keep = kept[0], kept[1]
        levels = rat[:, groups : 2 * groups, :]
        top = jnp.maximum(jnp.max(levels, axis=0), own_keep)
        share = jnp.exp(levels - top[None])
        mine = jnp.exp(own_keep - top)
        upper = jnp.sum(share * rat[:, 0:groups, :], axis=0) + mine * v_keep
        joined = upper / (jnp.sum(share, axis=0) + mine)
        ab[my_seq] = joined.astype(BF16).astype(F32)
        to_all_kv(ab, my_seq, K_ATT)

    got_kv(bb, K_B)
    squares = jnp.zeros((seqs, LANES), F32)
    for k in range(n_kv):
        v = bb[k].astype(F32)
        squares = squares + v * v
    scale = 0.5 * lax.rsqrt(lane_sum(squares) / width + EPS)
    for k in range(n_kv):
        mid[k] = xb[k].astype(F32) + bb[k].astype(F32) * scale * gain(1, k)
    loads[12].wait()

    got_from_owners(ab, rsem.at[K_ATT])
    attended = jnp.concatenate([ab[0:seqs, j, :] for j in range(groups)], axis=1).astype(BF16)
    tm[tp] = nn(attended, wo[...]).astype(BF16)
    to_all_tp(tm, T_MIX)
    got_tp(tm, T_MIX)
    mb[kv] = tp_sum(tm).astype(BF16)
    to_all_kv(mb, kv, K_MIX)
    got_kv(mb, K_MIX)

    squares = jnp.zeros((seqs, LANES), F32)
    for k in range(n_kv):
        v = mb[k].astype(F32)
        squares = squares + v * v
    scale = lax.rsqrt(lane_sum(squares) / width + EPS)
    squares = jnp.zeros((seqs, LANES), F32)
    for k in range(n_kv):
        v = mid[k] + mb[k].astype(F32) * scale * gain(3, k)
        mid[k] = v
        squares = squares + v * v
    scale = lax.rsqrt(lane_sum(squares) / width + EPS)
    for k in range(n_kv):
        xn[:, k * LANES : (k + 1) * LANES] = (mid[k] * scale * gain(4, k)).astype(BF16)
    for i in range(13, 16):
        loads[i].wait()
    feed_forward(g2, l2, d2, pf2)
    to_kv_blocks(pf2, rf2, R_F2)
    got_kv(rf2, R_F2)
    tf2[tp] = block_sum(rf2).astype(BF16)
    to_all_tp(tf2, T_F2)
    got_tp(tf2, T_F2)
    bf = tp_sum(tf2).astype(BF16).astype(F32)

    eye = lax.broadcasted_iota(jnp.int32, (seqs, LANES), 0) == lane_s
    stb[kv] = jnp.sum(jnp.where(eye, lane_sum(bf * bf), 0.0), axis=0, keepdims=True)
    to_all_kv(stb, kv, K_STAT)
    got_kv(stb, K_STAT)
    line = functools.reduce(lambda a, k: a + stb[k], range(1, n_kv), stb[0])
    total = lane_sum(jnp.where(eye, jnp.broadcast_to(line, (seqs, LANES)), 0.0))
    scale = lax.rsqrt(total / width + EPS)
    final = (mid[kv] + 0.5 * (bf * scale * gain(5))).astype(BF16)
    out_ref[...] = nt(place, final).astype(BF16)

    for stage, buf in ((T_TOK, ttok), (T_F1, tf), (T_MIX, tm), (T_F2, tf2)):
        wait(ssem.at[stage], buf.at[pl.ds(0, n_tp - 1)])
    for stage, buf in ((K_TOK, xb), (R_F1, pf), (K_B, bb), (K_MIX, mb), (R_F2, pf2), (K_STAT, stb)):
        wait(ssem.at[stage], buf.at[pl.ds(0, n_kv - 1)])
    for stage, buf in ((R_TOKQ, sq1), (R_QKV, sqk), (R_ATT, sat)):
        got_from_owners(buf, ssem.at[stage])

    @pl.when(owns)
    def _():
        for stage, buf in ((K_Q, qb), (K_ATT, ab)):
            wait(ssem.at[stage], buf.at[pl.ds(0, n_kv - 1)])


def solution(mesh):
    n_kv, n_tp = mesh.shape["kv"], mesh.shape["tp"]
    axes = ("kv", "tp")

    def body(tokens, gains, g1, l1, d1, wq, wk, wv, wf, wo, g2, l2, d2, ck, cv, cd):
        seqs, own = tokens.shape
        width = own * n_kv * n_tp
        groups = cd.shape[1] * HD // LANES
        arrays = (tokens.T, gains, g1.T, l1.T, d1, wq, wk, wv, wf.T, wo, g2.T, l2.T, d2, ck, cv, cd)
        vm = pltpu.VMEM
        block = (seqs, LANES)
        pieces = (4 * groups, LANES)
        scratch = [vm(a.shape, a.dtype) for a in arrays] + [
            vm((n_tp, *block), BF16),
            vm((n_kv, *block), BF16),
            vm((seqs, width), BF16),
            vm((seqs, *pieces), F32),
            vm((seqs, *pieces), BF16),
            vm((n_kv, *pieces), BF16),
            vm((n_kv, *block), BF16),
            vm((n_kv, *block), BF16),
            vm((n_tp, *block), BF16),
            vm((seqs, *pieces), BF16),
            vm((n_kv, *pieces), BF16),
            vm((n_kv, *block), BF16),
            vm((n_kv, groups, LANES), F32),
            vm((seqs, 2 * groups, LANES), F32),
            vm((n_kv, 2 * groups, LANES), F32),
            vm((n_kv, groups, LANES), F32),
            vm((n_tp, *block), BF16),
            vm((n_kv, *block), BF16),
            vm((n_kv, *block), F32),
            vm((n_kv, *block), BF16),
            vm((n_kv, *block), BF16),
            vm((n_tp, *block), BF16),
            vm((n_kv, 1, LANES), F32),
            vm((2, groups, LANES), F32),
            pltpu.SemaphoreType.DMA((len(arrays),)),
            pltpu.SemaphoreType.DMA((STAGES,)),
            pltpu.SemaphoreType.DMA((STAGES,)),
        ]
        out = pl.pallas_call(
            functools.partial(kernel, n_kv, n_tp, seqs, width),
            out_shape=jax.ShapeDtypeStruct((own, seqs), BF16),
            in_specs=[pl.BlockSpec(memory_space=pl.ANY)] * len(arrays),
            out_specs=pl.BlockSpec(memory_space=pltpu.VMEM),
            scratch_shapes=scratch,
            compiler_params=pltpu.CompilerParams(
                collective_id=0, has_side_effects=True, vmem_limit_bytes=56 * 1024 * 1024
            ),
            name="layer",
        )(*arrays)
        return out.T

    placed = (
        P(None, axes), P(), P(None, axes), P(None, axes), P(axes, None), P("kv", "tp"), P("kv", "tp"), P("kv", "tp"),
        P(None, "tp"), P("tp", "kv"), P(None, axes), P(None, axes), P(axes, None), P(None, "kv", "tp"),
        P(None, "kv", "tp"), P(None, "tp", "kv"),
    )
    return jax.shard_map(body, mesh=mesh, in_specs=placed, out_specs=P(None, axes), check_vma=False)
```

```python
import functools

import jax
import jax.numpy as jnp
from jax import lax
from jax.experimental import pallas as pl
from jax.experimental.pallas import tpu as pltpu
from jax.sharding import PartitionSpec as P

MESH = pl.DeviceIdType.MESH
F32, BF16 = jnp.float32, jnp.bfloat16
EPS = 1e-06
HD = 64
LANES = 128
ROWS = 24
NX = 4
STAGES = 15
(T_TOK, K_TOK, R_TOKQ, R_F1, T_F1, R_QKV, K_B, K_Q, R_ATT, K_ATT, T_MIX, K_MIX, R_F2, T_F2, K_STAT) = range(STAGES)


def nt(a, b):
    return lax.dot_general(a, b, (((1,), (1,)), ((), ())), preferred_element_type=F32)


def nn(a, b):
    return jnp.dot(a, b, preferred_element_type=F32)


def lane_sum(v):
    return jnp.sum(v, axis=-1, keepdims=True)


def rows_of(ref, k):
    return ref[k].astype(F32).reshape(ROWS, LANES)


def put_rows(ref, k, v):
    ref[k] = v.reshape(ROWS // 8, 8, LANES).astype(BF16)


def padded(v):
    return jnp.concatenate([v, jnp.zeros((ROWS - v.shape[0], v.shape[1]), v.dtype)], axis=0)


def silu(v):
    return v / (1.0 + jnp.exp(-v))


def kernel(
    n_kv, n_tp, seqs, width,
    tok_h, gains_h, g1_h, l1_h, d1_h, wq_h, wk_h, wv_h, wf_h, wo_h, g2_h, l2_h, d2_h, ck_h, cv_h, cd_h,
    out_ref,
    tok, gains, g1, l1, d1, wq, wk, wv, wf, wo, g2, l2, d2, ck, cv, cd,
    ttok, xb, xn, piece, sq1, rq1, pf, rf, tf, sqk, rqk, bb, qb, sat, rat, ab, tm, mb, mid, pf2, rf2, tf2, stb, kept, sc, wt, sl, si,
    load_sem, ssem, rsem,
):
    kv, tp = lax.axis_index("kv"), lax.axis_index("tp")
    nz = n_kv // NX
    zz, xx = kv // NX, kv % NX
    col = pl.multiple_of(kv * LANES, LANES)
    heads = cd.shape[1]
    groups = heads * HD // LANES

    loads = [
        pltpu.make_async_copy(h, v, load_sem.at[i])
        for i, (h, v) in enumerate(
            [(tok_h, tok), (gains_h, gains), (wq_h, wq), (wk_h, wk), (wv_h, wv), (wf_h, wf), (g1_h, g1), (l1_h, l1),
             (d1_h, d1), (ck_h, ck), (cd_h, cd), (cv_h, cv), (wo_h, wo), (g2_h, g2), (l2_h, l2), (d2_h, d2)]
        )
    ]
    for copy in loads:
        copy.start()

    def owner_of(b):
        return (n_kv * b + seqs - 1) // seqs

    my_seq = (kv * seqs) // n_kv
    owns = owner_of(my_seq) == kv

    def kv_peer(i):
        a, c = i // NX, i % NX
        dz = (nz // 2 + ((a + 1) // 2) * (1 - 2 * (a % 2)) + nz) % nz
        dx = (NX // 2 + ((c + 1) // 2) * (1 - 2 * (c % 2)) + NX) % NX
        return ((zz + dz) % nz) * NX + (xx + dx) % NX

    def tp_peer(i):
        return (tp + 1 + i) % n_tp

    def send(src, dst, stage, **where):
        pltpu.make_async_remote_copy(
            src_ref=src, dst_ref=dst, send_sem=ssem.at[stage], recv_sem=rsem.at[stage],
            device_id=where, device_id_type=MESH,
        ).start()

    def wait(sem, ref):
        pltpu.make_async_copy(ref, ref, sem).wait()

    def to_all_kv(buf, slot, stage):
        @pl.loop(0, n_kv - 1)
        def _(i):
            send(buf.at[slot], buf.at[slot], stage, kv=kv_peer(i))

    def to_all_tp(buf, stage):
        @pl.loop(0, n_tp - 1)
        def _(i):
            send(buf.at[tp], buf.at[tp], stage, tp=tp_peer(i))

    def got_kv(buf, stage):
        wait(rsem.at[stage], buf.at[pl.ds(0, n_kv - 1)])

    def got_tp(buf, stage):
        wait(rsem.at[stage], buf.at[pl.ds(0, n_tp - 1)])

    def to_kv_blocks(src, dst, stage):
        @pl.loop(0, n_kv - 1)
        def _(i):
            k = kv_peer(i)
            send(src.at[k], dst.at[kv], stage, kv=k)

        dst[kv] = src[kv]

    def send_owner(src, dst, b, stage):
        @pl.when(owner_of(b) != kv)
        def _():
            send(src.at[b], dst.at[kv], stage, kv=owner_of(b))

    def to_owners(src, dst, stage):
        @pl.loop(0, seqs)
        def _(b):
            send_owner(src, dst, b, stage)

        @pl.when(owns)
        def _():
            dst[kv] = src[my_seq]

    def got_from_owners(buf, sem):
        @pl.when(owns)
        def _():
            wait(sem, buf.at[pl.ds(0, seqs - 1)])

        @pl.when(jnp.logical_not(owns))
        def _():
            wait(sem, buf.at[pl.ds(0, seqs)])

    barrier = pltpu.get_barrier_semaphore()

    @pl.loop(0, n_kv - 1)
    def _(i):
        pl.semaphore_signal(barrier, inc=1, device_id={"kv": kv_peer(i)}, device_id_type=MESH)

    @pl.loop(0, n_tp - 1)
    def _(i):
        pl.semaphore_signal(barrier, inc=1, device_id={"tp": tp_peer(i)}, device_id_type=MESH)

    loads[0].wait()
    own_w = tok.shape[0]
    lane = lax.broadcasted_iota(jnp.int32, (own_w, LANES), 1)
    row = lax.broadcasted_iota(jnp.int32, (own_w, LANES), 0)
    place = jnp.where(lane == row + own_w * tp, 1.0, 0.0).astype(BF16)
    put_rows(ttok, tp, padded(lax.dot_general(tok[...], place, (((0,), (0,)), ((), ())), preferred_element_type=F32)))
    ab[seqs:ROWS] = jnp.zeros((ROWS - seqs, groups, LANES), F32)

    pl.semaphore_wait(barrier, n_kv + n_tp - 2)

    def block_sum(buf):
        return functools.reduce(lambda a, k: a + rows_of(buf, k), range(1, n_kv), rows_of(buf, 0))

    def tp_sum(buf):
        return functools.reduce(lambda a, k: a + rows_of(buf, k), range(1, n_tp), rows_of(buf, 0))

    def piece_sum(buf):
        return functools.reduce(lambda a, k: a + buf[k].astype(F32), range(1, n_kv), buf[0].astype(F32))

    to_all_tp(ttok, T_TOK)
    got_tp(ttok, T_TOK)
    tblk = tp_sum(ttok)
    put_rows(xb, kv, tblk)
    to_all_kv(xb, kv, K_TOK)

    for i in range(1, 6):
        loads[i].wait()

    def gain(i, k=None):
        return gains[i : i + 1, pl.ds(col, LANES)] if k is None else gains[i : i + 1, k * LANES : (k + 1) * LANES]

    lane_s = lax.broadcasted_iota(jnp.int32, (ROWS, LANES), 1)

    def projections(x, stats, out):
        parts = [nn(x, w[...]) for w in (wq, wk, wv)]
        for i, part in enumerate(parts):
            for j in range(groups):
                piece[:, i * groups + j, :] = part[0:seqs, j * LANES : (j + 1) * LANES]
        gates = nt(x, wf[:, pl.ds(col, LANES)])
        for j in range(groups):
            line = jnp.where(lane_s == 0, gates[:, 2 * j : 2 * j + 1], 0.0)
            line = line + jnp.where(lane_s == HD, gates[:, 2 * j + 1 : 2 * j + 2], 0.0)
            if j == 0:
                for n, stat in enumerate(stats):
                    high = stat.astype(BF16).astype(F32)
                    line = line + jnp.where(lane_s == n + 1, high, 0.0)
                    line = line + jnp.where(lane_s == HD + n + 1, stat - high, 0.0)
            piece[:, 3 * groups + j, :] = line[0:seqs]
        out[...] = piece[...].astype(BF16)

    projections((tblk * gain(2)).astype(BF16), [lane_sum(tblk * tblk)], sq1)
    to_owners(sq1, rq1, R_TOKQ)

    def feed_forward(gate_w, lift_w, down_w, part_out):
        x = xn[...]
        act = (silu(nt(x, gate_w[...])) * nt(x, lift_w[...])).astype(BF16)
        for c in range(0, n_kv, 4):
            part = nn(act, down_w[:, c * LANES : (c + 4) * LANES])
            for j in range(4):
                put_rows(part_out, c + j, part[:, j * LANES : (j + 1) * LANES])

    got_kv(xb, K_TOK)
    squares = jnp.zeros((ROWS, LANES), F32)
    for k in range(n_kv):
        v = rows_of(xb, k)
        squares = squares + v * v
    scale = lax.rsqrt(lane_sum(squares) / width + EPS)
    for k in range(n_kv):
        xn[:, k * LANES : (k + 1) * LANES] = (rows_of(xb, k) * scale * gain(0, k)).astype(BF16)
    for i in range(6, 9):
        loads[i].wait()
    feed_forward(g1, l1, d1, pf)
    to_kv_blocks(pf, rf, R_F1)
    got_kv(rf, R_F1)
    put_rows(tf, tp, block_sum(rf))
    to_all_tp(tf, T_F1)
    got_tp(tf, T_F1)
    put_rows(bb, kv, tp_sum(tf))
    bf = rows_of(bb, kv)
    u = bf * gain(1)
    projections((u * gain(2)).astype(BF16), [lane_sum(bf * bf), lane_sum(tblk * u), lane_sum(u * u)], sqk)
    to_owners(sqk, rqk, R_QKV)

    low = lax.broadcasted_iota(jnp.int32, (groups, LANES), 1) < HD

    def halves(a, b):
        return jnp.where(low, a, b)

    lane_1 = lax.broadcasted_iota(jnp.int32, (1, LANES), 1)

    def stat_of(line, n):
        return lane_sum(jnp.where((lane_1 == n + 1) | (lane_1 == HD + n + 1), line, 0.0))

    def own_rows():
        asum, bsum = piece_sum(rq1), piece_sum(rqk)
        at, bt = 3 * groups, 3 * groups + 1
        s_b, s_tu, s_uu = [stat_of(bsum[at:bt], n) for n in range(3)]
        r1 = lax.rsqrt(s_b / width + EPS)
        s_mid = stat_of(asum[at:bt], 0) + r1 * s_tu + 0.25 * r1 * r1 * s_uu
        scale_mid = lax.rsqrt(s_mid / width + EPS)
        full = scale_mid * (asum + 0.5 * r1 * bsum)
        q, k, v, f = [full[i * groups : (i + 1) * groups] for i in range(4)]
        q, k, v = [t.astype(BF16).astype(F32) for t in (q, k, v)]
        f = halves(f[:, 0:1], f[:, HD : HD + 1])
        forget = jnp.minimum(f, 0.0) - jnp.log(1.0 + jnp.exp(-jnp.abs(f)))
        qk = q * k
        own = halves(lane_sum(jnp.where(low, qk, 0.0)), lane_sum(jnp.where(low, 0.0, qk))) * (HD**-0.5) - forget
        return q, own, v

    @pl.when(owns)
    def _():
        got_kv(rq1, R_TOKQ)
        got_kv(rqk, R_QKV)
        q, own, v = own_rows()
        qb[my_seq] = q
        kept[0] = own
        kept[1] = v
        to_all_kv(qb, my_seq, K_Q)

    got_from_owners(qb, rsem.at[K_Q])
    to_all_kv(bb, kv, K_B)

    for i in range(9, 12):
        loads[i].wait()
    head_i = lax.broadcasted_iota(jnp.int32, (heads, LANES), 0)
    lane_h = lax.broadcasted_iota(jnp.int32, (heads, LANES), 1)
    masks = [head_i == 2 * j + lane_h // HD for j in range(groups)]

    batch = 6

    @pl.loop(0, seqs, step=batch)
    def _(first):
        for i in range(batch):
            b = first + i
            rows = [jnp.where(masks[j], jnp.broadcast_to(qb[b, j : j + 1, :], (heads, LANES)), 0.0) for j in range(groups)]
            query = jnp.concatenate(rows, axis=1).astype(BF16)
            sc[b] = nt(query, ck[b]) * (HD**-0.5) + cd[b]

    score = sc[...]
    peak = jnp.max(score, axis=2, keepdims=True)
    raised = jnp.exp(score - peak)
    total = jnp.sum(raised, axis=2, keepdims=True)
    wt[...] = raised.astype(BF16)
    sl[...] = jnp.broadcast_to(peak + jnp.log(total), (seqs, heads, LANES))
    si[...] = jnp.broadcast_to(1.0 / total, (seqs, heads, LANES))

    @pl.loop(0, seqs, step=batch)
    def _(first):
        for i in range(batch):
            b = first + i
            o = nn(wt[b], cv[b])
            level, part = sl[b], si[b]
            for j in range(groups):
                oj = jnp.where(masks[j], o[:, j * LANES : (j + 1) * LANES] * part, 0.0)
                sat[b, j : j + 1, :] = jnp.sum(oj, axis=0, keepdims=True)
                lj = jnp.where(masks[j], level, 0.0)
                sat[b, groups + j : groups + j + 1, :] = jnp.sum(lj, axis=0, keepdims=True)
            send_owner(sat, rat, b, R_ATT)

    @pl.when(owns)
    def _():
        rat[kv] = sat[my_seq]
        got_kv(rat, R_ATT)
        own_keep, v_keep = kept[0], kept[1]
        levels = rat[:, groups : 2 * groups, :]
        top = jnp.maximum(jnp.max(levels, axis=0), own_keep)
        share = jnp.exp(levels - top[None])
        mine = jnp.exp(own_keep - top)
        upper = jnp.sum(share * rat[:, 0:groups, :], axis=0) + mine * v_keep
        joined = upper / (jnp.sum(share, axis=0) + mine)
        ab[my_seq] = joined.astype(BF16).astype(F32)
        to_all_kv(ab, my_seq, K_ATT)

    got_kv(bb, K_B)
    squares = jnp.zeros((ROWS, LANES), F32)
    for k in range(n_kv):
        v = rows_of(bb, k)
        squares = squares + v * v
    scale = 0.5 * lax.rsqrt(lane_sum(squares) / width + EPS)
    for k in range(n_kv):
        mid[k] = rows_of(xb, k) + rows_of(bb, k) * scale * gain(1, k)
    loads[12].wait()

    got_from_owners(ab, rsem.at[K_ATT])
    attended = jnp.concatenate([ab[0:ROWS, j, :] for j in range(groups)], axis=1).astype(BF16)
    put_rows(tm, tp, nn(attended, wo[...]))
    to_all_tp(tm, T_MIX)
    got_tp(tm, T_MIX)
    put_rows(mb, kv, tp_sum(tm))
    to_all_kv(mb, kv, K_MIX)
    got_kv(mb, K_MIX)

    squares = jnp.zeros((ROWS, LANES), F32)
    for k in range(n_kv):
        v = rows_of(mb, k)
        squares = squares + v * v
    scale = lax.rsqrt(lane_sum(squares) / width + EPS)
    squares = jnp.zeros((ROWS, LANES), F32)
    for k in range(n_kv):
        v = mid[k] + rows_of(mb, k) * scale * gain(3, k)
        mid[k] = v
        squares = squares + v * v
    scale = lax.rsqrt(lane_sum(squares) / width + EPS)
    for k in range(n_kv):
        xn[:, k * LANES : (k + 1) * LANES] = (mid[k] * scale * gain(4, k)).astype(BF16)
    for i in range(13, 16):
        loads[i].wait()
    feed_forward(g2, l2, d2, pf2)
    to_kv_blocks(pf2, rf2, R_F2)
    got_kv(rf2, R_F2)
    put_rows(tf2, tp, block_sum(rf2))
    to_all_tp(tf2, T_F2)
    got_tp(tf2, T_F2)
    bf = tp_sum(tf2)

    eye = lax.broadcasted_iota(jnp.int32, (ROWS, LANES), 0) == lane_s
    stb[kv] = jnp.sum(jnp.where(eye, lane_sum(bf * bf), 0.0), axis=0, keepdims=True)
    to_all_kv(stb, kv, K_STAT)
    got_kv(stb, K_STAT)
    line = functools.reduce(lambda a, k: a + stb[k], range(1, n_kv), stb[0])
    total = lane_sum(jnp.where(eye, jnp.broadcast_to(line, (ROWS, LANES)), 0.0))
    scale = lax.rsqrt(total / width + EPS)
    final = (mid[kv] + 0.5 * (bf * scale * gain(5))).astype(BF16)
    out_ref[...] = nt(place, final)[:, 0:seqs].astype(BF16)

    for stage, buf in ((T_TOK, ttok), (T_F1, tf), (T_MIX, tm), (T_F2, tf2)):
        wait(ssem.at[stage], buf.at[pl.ds(0, n_tp - 1)])
    for stage, buf in ((K_TOK, xb), (R_F1, pf), (K_B, bb), (K_MIX, mb), (R_F2, pf2), (K_STAT, stb)):
        wait(ssem.at[stage], buf.at[pl.ds(0, n_kv - 1)])
    for stage, buf in ((R_TOKQ, sq1), (R_QKV, sqk), (R_ATT, sat)):
        got_from_owners(buf, ssem.at[stage])

    @pl.when(owns)
    def _():
        for stage, buf in ((K_Q, qb), (K_ATT, ab)):
            wait(ssem.at[stage], buf.at[pl.ds(0, n_kv - 1)])


def solution(mesh):
    n_kv, n_tp = mesh.shape["kv"], mesh.shape["tp"]
    axes = ("kv", "tp")

    def body(tokens, gains, g1, l1, d1, wq, wk, wv, wf, wo, g2, l2, d2, ck, cv, cd):
        seqs, own = tokens.shape
        width = own * n_kv * n_tp
        groups = cd.shape[1] * HD // LANES
        arrays = (tokens.T, gains, g1.T, l1.T, d1, wq, wk, wv, wf.T, wo, g2.T, l2.T, d2, ck, cv, cd)
        vm = pltpu.VMEM
        block = (ROWS // 8, 8, LANES)
        heads = cd.shape[1]
        pieces = (4 * groups, LANES)
        scratch = [vm(a.shape, a.dtype) for a in arrays] + [
            vm((n_tp, *block), BF16),
            vm((n_kv, *block), BF16),
            vm((ROWS, width), BF16),
            vm((seqs, *pieces), F32),
            vm((seqs, *pieces), BF16),
            vm((n_kv, *pieces), BF16),
            vm((n_kv, *block), BF16),
            vm((n_kv, *block), BF16),
            vm((n_tp, *block), BF16),
            vm((seqs, *pieces), BF16),
            vm((n_kv, *pieces), BF16),
            vm((n_kv, *block), BF16),
            vm((n_kv, groups, LANES), F32),
            vm((seqs, 2 * groups, LANES), F32),
            vm((n_kv, 2 * groups, LANES), F32),
            vm((n_kv, groups, LANES), F32),
            vm((n_tp, *block), BF16),
            vm((n_kv, *block), BF16),
            vm((n_kv, ROWS, LANES), F32),
            vm((n_kv, *block), BF16),
            vm((n_kv, *block), BF16),
            vm((n_tp, *block), BF16),
            vm((n_kv, 1, LANES), F32),
            vm((2, groups, LANES), F32),
            vm((seqs, heads, cd.shape[2]), F32),
            vm((seqs, heads, cd.shape[2]), BF16),
            vm((seqs, heads, LANES), F32),
            vm((seqs, heads, LANES), F32),
            pltpu.SemaphoreType.DMA((len(arrays),)),
            pltpu.SemaphoreType.DMA((STAGES,)),
            pltpu.SemaphoreType.DMA((STAGES,)),
        ]
        out = pl.pallas_call(
            functools.partial(kernel, n_kv, n_tp, seqs, width),
            out_shape=jax.ShapeDtypeStruct((own, seqs), BF16),
            in_specs=[pl.BlockSpec(memory_space=pl.ANY)] * len(arrays),
            out_specs=pl.BlockSpec(memory_space=pltpu.VMEM),
            scratch_shapes=scratch,
            compiler_params=pltpu.CompilerParams(
                collective_id=0, has_side_effects=True, vmem_limit_bytes=56 * 1024 * 1024
            ),
            name="layer",
        )(*arrays)
        return out.T

    placed = (
        P(None, axes), P(), P(None, axes), P(None, axes), P(axes, None), P("kv", "tp"), P("kv", "tp"), P("kv", "tp"),
        P(None, "tp"), P("tp", "kv"), P(None, axes), P(None, axes), P(axes, None), P(None, "kv", "tp"),
        P(None, "kv", "tp"), P(None, "tp", "kv"),
    )
    return jax.shard_map(body, mesh=mesh, in_specs=placed, out_specs=P(None, axes), check_vma=False)
```

```python
import functools

import jax
import jax.numpy as jnp
from jax import lax
from jax.experimental import pallas as pl
from jax.experimental.pallas import tpu as pltpu
from jax.sharding import PartitionSpec as P

MESH = pl.DeviceIdType.MESH
F32, BF16 = jnp.float32, jnp.bfloat16
EPS = 1e-06
HD = 64
LANES = 128
ROWS = 24
TILE = 32
NX = 4
STAGES = 21
(T_TOK, K_TOK, X_W, X_WO, R_F1, P_F1, K_QA, K_QB, O_A, O_B, Z_ST, Z_OWN, Z_OWNL, K_B, R_ATT, R_LSE, P_MIX, K_MIX,
 R_F2, T_F2, K_STAT) = range(STAGES)


def nt(a, b):
    return lax.dot_general(a, b, (((1,), (1,)), ((), ())), preferred_element_type=F32)


def nn(a, b):
    return jnp.dot(a, b, preferred_element_type=F32)


def lane_sum(v):
    return jnp.sum(v, axis=-1, keepdims=True)


def rows_of(ref, k):
    return ref[k, 0:ROWS, :].astype(F32)


def put_rows(ref, k, v):
    ref[k, 0:ROWS, :] = v.astype(BF16)


def total_of(buf, slots):
    slots = list(slots)
    return functools.reduce(lambda a, k: a + rows_of(buf, k), slots[1:], rows_of(buf, slots[0]))


def padded(v):
    return jnp.concatenate([v, jnp.zeros((ROWS - v.shape[0], v.shape[1]), v.dtype)], axis=0)


def silu(v):
    return v / (1.0 + jnp.exp(-v))


def kernel(
    n_kv, n_tp, seqs, width,
    tok_h, gains_h, wq_h, wk_h, wv_h, wf_h, g1_h, l1_h, d1_h, ck_h, cd_h, cv_h, wo_h, g2_h, l2_h, d2_h,
    out_ref,
    tok, gains, wq, wk, wv, wf, g1, l1, d1, ck, cd, cv, wo, g2, l2, d2,
    ttok, xb, xn, wx, wo2, pf, rf, pb, bb, qa, qb, oa, ob, roa, rob, zst, qf, sc, wt, si, om, so, ls, ro, rl, wsq,
    sm, rm, mb, mid, pf2, rf2, tf2, stb,
    load_sem, ssem, rsem, hello,
):
    kv, tp = lax.axis_index("kv"), lax.axis_index("tp")
    nz = n_kv // NX
    zz, xx = kv // NX, kv % NX
    n_plane = NX * n_tp
    me = xx * n_tp + tp
    heads = cd.shape[1]
    groups = heads * HD // LANES
    zwide = NX * LANES
    zcol = pl.multiple_of(zz * zwide, LANES)
    xcol = pl.multiple_of(xx * LANES, LANES)
    col = pl.multiple_of(kv * LANES, LANES)

    loads = [
        pltpu.make_async_copy(h, v, load_sem.at[i])
        for i, (h, v) in enumerate(
            [(tok_h, tok), (gains_h, gains), (wq_h, wq), (wk_h, wk), (wv_h, wv), (wf_h, wf), (g1_h, g1), (l1_h, l1),
             (d1_h, d1), (ck_h, ck), (cd_h, cd), (cv_h, cv), (wo_h, wo), (g2_h, g2), (l2_h, l2), (d2_h, d2)]
        )
    ]
    for copy in loads:
        copy.start()

    def ordered(i, n):
        return (n // 2 + ((i + 1) // 2) * (1 - 2 * (i % 2)) + n) % n

    def kv_at(dz, dx):
        return ((zz + dz + nz) % nz) * NX + (xx + dx) % NX

    def kv_peer(i):
        return kv_at(ordered(i // NX, nz), ordered(i % NX, NX))

    def tp_peer(i):
        return (tp + 1 + i) % n_tp

    def plane_peer(i):
        return (xx + ordered(i // n_tp, NX)) % NX, (tp + 1 + i % n_tp) % n_tp

    def at(x):
        return zz * NX + x

    z_own = (2 * xx + tp) % nz
    owns = zz == z_own

    def send(src, dst, stage, **where):
        pltpu.make_async_remote_copy(
            src_ref=src, dst_ref=dst, send_sem=ssem.at[stage], recv_sem=rsem.at[stage],
            device_id=where, device_id_type=MESH,
        ).start()

    def wait(sem, ref):
        pltpu.make_async_copy(ref, ref, sem).wait()

    def part(buf, slot):
        if buf.shape[-2] != TILE:
            return buf.at[slot]
        if len(buf.shape) == 4:
            return buf.at[slot, :, pl.ds(0, seqs)]
        return buf.at[slot, pl.ds(0, seqs)]

    def got(stage, buf, n):
        wait(rsem.at[stage], part(buf, pl.ds(0, n)))

    def gone(stage, buf, n):
        wait(ssem.at[stage], part(buf, pl.ds(0, n)))

    def to_all_kv(buf, stage, count=n_kv - 1):
        @pl.loop(0, count)
        def _(i):
            send(part(buf, kv), part(buf, kv), stage, kv=kv_peer(i))

    def to_all_tp(buf, stage):
        @pl.loop(0, n_tp - 1)
        def _(i):
            send(part(buf, tp), part(buf, tp), stage, tp=tp_peer(i))

    def to_all_z(buf, slot, stage):
        @pl.loop(0, nz - 1)
        def _(i):
            send(part(buf, slot), part(buf, slot), stage, kv=kv_at(ordered(i, nz), 0))

    def to_kv_blocks(src, dst, stage):
        @pl.loop(0, n_kv - 1)
        def _(i):
            k = kv_peer(i)
            send(part(src, k), part(dst, kv), stage, kv=k)

        dst[kv] = src[kv]

    barrier = pltpu.get_barrier_semaphore()
    for i in range(n_tp - 1):
        pl.semaphore_signal(barrier, inc=1, device_id={"tp": tp_peer(i)}, device_id_type=MESH)
    for dz, dx in [(0, d) for d in range(1, NX)] + [(1, 0), (-1, 0)]:
        pl.semaphore_signal(barrier, inc=1, device_id={"kv": kv_at(dz, dx)}, device_id_type=MESH)

    loads[0].wait()
    own_w = tok.shape[0]
    lane = lax.broadcasted_iota(jnp.int32, (own_w, LANES), 1)
    row = lax.broadcasted_iota(jnp.int32, (own_w, LANES), 0)
    place = jnp.where(lane == row + own_w * tp, 1.0, 0.0).astype(BF16)
    mine = lax.dot_general(tok[...], place, (((0,), (0,)), ((), ())), preferred_element_type=F32)
    put_rows(ttok, tp, padded(mine))

    pl.semaphore_wait(barrier, n_tp - 1 + NX - 1 + 2)

    to_all_tp(ttok, T_TOK)
    for i in range(2, 5):
        loads[i].wait()
    for d in range(1, NX):
        j = (xx + d) % NX
        for m, w in enumerate((wq, wk, wv)):
            send(w.at[:, pl.ds(pl.multiple_of(j * LANES, LANES), LANES)], wx.at[m, xx], X_W, kv=at(j))
    for m, w in enumerate((wq, wk, wv)):
        wx[m, xx] = w[:, pl.ds(xcol, LANES)]
    for n, step in enumerate((1, 2, 1)):
        for dz in (step, -step):
            pl.semaphore_signal(hello.at[n], inc=1, device_id={"kv": kv_at(dz, 0)}, device_id_type=MESH)
        pl.semaphore_wait(hello.at[n], 2)
    got(T_TOK, ttok, n_tp - 1)
    put_rows(xb, kv, total_of(ttok, range(n_tp)))
    to_all_kv(xb, K_TOK)

    def gain(i, k):
        return gains[i : i + 1, k * LANES : (k + 1) * LANES]

    def zgain(i):
        return gains[i : i + 1, pl.ds(zcol, zwide)]

    def feed_forward(gate_w, lift_w, down_w, part_out):
        x = xn[...]
        act = (silu(nt(x, gate_w[...])) * nt(x, lift_w[...])).astype(BF16)
        for c in range(0, n_kv, 4):
            some = nn(act, down_w[:, c * LANES : (c + 4) * LANES])
            for j in range(4):
                put_rows(part_out, c + j, some[:, j * LANES : (j + 1) * LANES])

    lane_r = lax.broadcasted_iota(jnp.int32, (ROWS, LANES), 1)
    low = lane_r < HD
    eye = lax.broadcasted_iota(jnp.int32, (ROWS, LANES), 0) == lane_r

    def flat(column):
        return jnp.sum(jnp.where(eye, column, 0.0), axis=0, keepdims=True)

    def upright(line):
        return lane_sum(jnp.where(eye, jnp.broadcast_to(line, (ROWS, LANES)), 0.0))

    loads[1].wait()
    got(K_TOK, xb, n_kv - 1)
    squares = jnp.zeros((ROWS, LANES), F32)
    for k in range(n_kv):
        v = rows_of(xb, k)
        squares = squares + v * v
    s_tt = lane_sum(squares)
    scale = lax.rsqrt(s_tt / width + EPS)
    for k in range(n_kv):
        xn[:, k * LANES : (k + 1) * LANES] = (rows_of(xb, k) * scale * gain(0, k)).astype(BF16)
    for i in range(6, 9):
        loads[i].wait()
    feed_forward(g1, l1, d1, pf)
    to_kv_blocks(pf, rf, R_F1)

    loads[5].wait()
    wait(rsem.at[X_W], wx.at[:, pl.ds(0, NX - 1)])
    tz = jnp.concatenate([rows_of(xb, at(x)) for x in range(NX)], axis=1)
    lane_f = lax.broadcasted_iota(jnp.int32, (ROWS, heads), 1)

    def projections(x, q_out, o_out):
        q, k, v = [nn(x, wx[m].reshape(zwide, LANES)) for m in range(3)]
        f = nt(x, wf[:, pl.ds(zcol, zwide)])
        f0, f1 = [lane_sum(jnp.where(lane_f == 2 * xx + g, f, 0.0)) for g in range(2)]
        put_rows(q_out, kv, q)
        put_rows(o_out, 0, k)
        put_rows(o_out, 1, v)
        put_rows(o_out, 2, jnp.where(low, f0, f1))

    def to_owner(src, dst, stage):
        whole = src.at[:, pl.ds(0, seqs)]

        @pl.when(jnp.logical_not(owns))
        def _():
            send(whole, dst.at[zz, :, pl.ds(0, seqs)], stage, kv=z_own * NX + xx)

        @pl.when(owns)
        def _():
            dst[zz] = src[...]

    projections((tz * zgain(2)).astype(BF16), qa, oa)

    got(R_F1, rf, n_kv - 1)
    put_rows(pb, me, total_of(rf, range(n_kv)))

    def to_plane(src, dst, stage, pick):
        @pl.loop(0, n_plane - 1)
        def _(i):
            x, t = plane_peer(i)
            send(part(src, pick(x)), part(dst, me), stage, kv=at(x), tp=t)

    to_plane(pb, pb, P_F1, lambda x: me)
    to_all_kv(qa, K_QA)
    to_owner(oa, roa, O_A)

    got(P_F1, pb, n_plane - 1)
    for x in range(NX):
        put_rows(bb, at(x), total_of(pb, range(x * n_tp, (x + 1) * n_tp)))
    bz = jnp.concatenate([rows_of(bb, at(x)) for x in range(NX)], axis=1)
    u = bz * zgain(1)
    projections((u * zgain(2)).astype(BF16), qb, ob)
    to_all_kv(qb, K_QB)
    for n, stat in enumerate((bz * bz, tz * u, u * u)):
        zst[zz, n : n + 1, :] = flat(lane_sum(stat))
    to_all_z(zst, zz, Z_ST)
    to_owner(ob, rob, O_B)

    got(K_QA, qa, n_kv - 1)
    got(Z_ST, zst, nz - 1)
    stats = functools.reduce(lambda a, z: a + zst[z], range(1, nz), zst[0])
    s_bb, s_tu, s_uu = [upright(stats[n : n + 1]) for n in range(3)]
    r1 = lax.rsqrt(s_bb / width + EPS)
    half = 0.5 * r1
    scale_mid = lax.rsqrt((s_tt + r1 * s_tu + half * half * s_uu) / width + EPS)
    got(K_QB, qb, n_kv - 1)
    for j in range(groups):
        slots = range(j, n_kv, NX)
        qf[j] = (scale_mid * (total_of(qa, slots) + half * total_of(qb, slots))).astype(BF16).astype(F32)

    to_all_kv(bb, K_B, n_kv - NX)
    loads[12].wait()
    for d in range(1, NX):
        j = (xx + d) % NX
        send(wo.at[pl.ds(pl.multiple_of(j * LANES, LANES), LANES), :], wo2.at[xx], X_WO, kv=at(j))
    wo2[xx] = wo[pl.ds(xcol, LANES), :]
    for i in range(9, 12):
        loads[i].wait()
    head_i = lax.broadcasted_iota(jnp.int32, (heads, LANES), 0)
    lane_h = lax.broadcasted_iota(jnp.int32, (heads, LANES), 1)
    masks = [head_i == 2 * j + lane_h // HD for j in range(groups)]
    batch = 6

    @pl.loop(0, seqs, step=batch)
    def _(first):
        for i in range(batch):
            b = first + i
            rows = [
                jnp.where(masks[j], jnp.broadcast_to(qf[j, pl.ds(b, 1), :], (heads, LANES)), 0.0) for j in range(groups)
            ]
            query = jnp.concatenate(rows, axis=1).astype(BF16)
            sc[b] = nt(query, ck[b]) * (HD**-0.5) + cd[b]

    score = sc[...]
    peak = jnp.max(score, axis=2, keepdims=True)
    raised = jnp.exp(score - peak)
    total = jnp.sum(raised, axis=2, keepdims=True)
    wt[...] = raised.astype(BF16)
    si[...] = jnp.broadcast_to(1.0 / total, (seqs, heads, LANES))
    level = jnp.broadcast_to(peak + jnp.log(total), (seqs, heads, LANES))
    turn = lax.broadcasted_iota(jnp.int32, (seqs, heads, LANES), 0) == lax.broadcasted_iota(
        jnp.int32, (seqs, heads, LANES), 2
    )
    lines = jnp.sum(jnp.where(turn, level, 0.0), axis=0)
    for j in range(groups):
        ls[j] = lines[2 * j : 2 * j + 2]

    @pl.loop(0, seqs, step=batch)
    def _(first):
        for i in range(batch):
            b = first + i
            o = nn(wt[b], cv[b])
            share = si[b]
            here = pl.ds(pl.multiple_of(b * heads, heads), heads)
            for j in range(groups):
                om[here, j * LANES : (j + 1) * LANES] = jnp.where(masks[j], o[:, j * LANES : (j + 1) * LANES] * share, 0.0)

    pick = lax.broadcasted_iota(jnp.int32, (ROWS, seqs * heads), 1) // heads
    pick = jnp.where(pick == lax.broadcasted_iota(jnp.int32, (ROWS, seqs * heads), 0), 1.0, 0.0).astype(BF16)
    outs = nn(pick, om[...].astype(BF16))
    for j in range(groups):
        put_rows(so, j, outs[:, j * LANES : (j + 1) * LANES])

    @pl.loop(0, n_kv - 1)
    def _(i):
        k = kv_peer(i)
        send(ls.at[k % NX], rl.at[kv], R_LSE, kv=k)
        send(part(so, k % NX), part(ro, kv), R_ATT, kv=k)

    ro[kv] = so[xx]
    rl[kv] = ls[xx]

    @pl.when(owns)
    def _():
        got(O_A, roa, nz - 1)
        got(O_B, rob, nz - 1)

        def finished(n):
            a = functools.reduce(lambda t, z: t + roa[z, n, 0:ROWS, :].astype(F32), range(1, nz), roa[0, n, 0:ROWS, :].astype(F32))
            b = functools.reduce(lambda t, z: t + rob[z, n, 0:ROWS, :].astype(F32), range(1, nz), rob[0, n, 0:ROWS, :].astype(F32))
            return scale_mid * (a + half * b)

        k, v, f = [finished(n) for n in range(3)]
        qk = qf[xx] * k.astype(BF16).astype(F32)
        forget = jnp.minimum(f, 0.0) - jnp.log(1.0 + jnp.exp(-jnp.abs(f)))
        own0 = lane_sum(jnp.where(low, qk, 0.0)) * (HD**-0.5) - forget[:, 0:1]
        own1 = lane_sum(jnp.where(low, 0.0, qk)) * (HD**-0.5) - forget[:, HD : HD + 1]
        put_rows(ro, n_kv, v)
        rl[n_kv, 0:1, :] = flat(own0)
        rl[n_kv, 1:2, :] = flat(own1)
        to_all_z(rl, n_kv, Z_OWNL)
        to_all_z(ro, n_kv, Z_OWN)

    got(K_B, bb, n_kv - NX)
    for k in range(n_kv):
        mid[k] = rows_of(xb, k) + rows_of(bb, k) * half * gain(1, k)

    @pl.when(jnp.logical_not(owns))
    def _():
        wait(rsem.at[Z_OWNL], rl.at[n_kv])
        wait(rsem.at[Z_OWN], part(ro, n_kv))

    got(R_LSE, rl, n_kv - 1)
    n_src = n_kv + 1
    top = functools.reduce(jnp.maximum, [rl[s] for s in range(n_src)])
    raised = [jnp.exp(rl[s] - top) for s in range(n_src)]
    norm = 1.0 / functools.reduce(lambda a, b: a + b, raised)
    for s in range(n_src):
        wsq[2 * s : 2 * s + 2, :] = raised[s] * norm
    weights = wsq[...].T[0:ROWS]
    got(R_ATT, ro, n_kv - 1)
    joined = jnp.zeros((ROWS, LANES), F32)
    for s in range(n_src):
        joined = joined + jnp.where(low, weights[:, 2 * s : 2 * s + 1], weights[:, 2 * s + 1 : 2 * s + 2]) * rows_of(ro, s)
    attended = joined.astype(BF16)
    wait(rsem.at[X_WO], wo2.at[pl.ds(0, NX - 1)])
    for x in range(NX):
        put_rows(sm, x, nn(attended, wo2[x]))

    to_plane(sm, rm, P_MIX, lambda x: x)
    rm[me] = sm[xx]
    got(P_MIX, rm, n_plane - 1)
    put_rows(mb, kv, total_of(rm, range(n_plane)))

    to_all_kv(mb, K_MIX)
    for i in range(13, 16):
        loads[i].wait()

    got(K_MIX, mb, n_kv - 1)

    squares = jnp.zeros((ROWS, LANES), F32)
    for k in range(n_kv):
        v = rows_of(mb, k)
        squares = squares + v * v
    scale = lax.rsqrt(lane_sum(squares) / width + EPS)
    squares = jnp.zeros((ROWS, LANES), F32)
    for k in range(n_kv):
        v = mid[k] + rows_of(mb, k) * scale * gain(3, k)
        mid[k] = v
        squares = squares + v * v
    scale = lax.rsqrt(lane_sum(squares) / width + EPS)
    for k in range(n_kv):
        xn[:, k * LANES : (k + 1) * LANES] = (mid[k] * scale * gain(4, k)).astype(BF16)
    feed_forward(g2, l2, d2, pf2)
    to_kv_blocks(pf2, rf2, R_F2)
    got(R_F2, rf2, n_kv - 1)
    put_rows(tf2, tp, total_of(rf2, range(n_kv)))
    to_all_tp(tf2, T_F2)
    got(T_F2, tf2, n_tp - 1)
    bf = total_of(tf2, range(n_tp))

    stb[kv] = flat(lane_sum(bf * bf))
    to_all_kv(stb, K_STAT)
    got(K_STAT, stb, n_kv - 1)
    line = functools.reduce(lambda a, k: a + stb[k], range(1, n_kv), stb[0])
    scale = lax.rsqrt(upright(line) / width + EPS)
    final = (mid[kv] + 0.5 * (bf * scale * gains[5:6, pl.ds(col, LANES)])).astype(BF16)
    out_ref[...] = nt(place, final)[:, 0:seqs].astype(BF16)

    for stage, buf, n in (
        (T_TOK, ttok, n_tp - 1), (T_F2, tf2, n_tp - 1), (K_TOK, xb, n_kv - 1), (R_F1, pf, n_kv - 1), (P_F1, pb, n_plane - 1),
        (K_QA, qa, n_kv - 1), (K_QB, qb, n_kv - 1), (Z_ST, zst, nz - 1), (K_B, bb, n_kv - NX), (R_ATT, ro, n_kv - 1),
        (R_LSE, rl, n_kv - 1), (P_MIX, rm, n_plane - 1), (K_MIX, mb, n_kv - 1), (R_F2, pf2, n_kv - 1), (K_STAT, stb, n_kv - 1),
    ):
        gone(stage, buf, n)
    wait(ssem.at[X_W], wx.at[:, pl.ds(0, NX - 1)])
    wait(ssem.at[X_WO], wo2.at[pl.ds(0, NX - 1)])

    @pl.when(owns)
    def _():
        gone(Z_OWNL, rl, nz - 1)
        gone(Z_OWN, ro, nz - 1)

    @pl.when(jnp.logical_not(owns))
    def _():
        wait(ssem.at[O_A], oa.at[:, pl.ds(0, seqs)])
        wait(ssem.at[O_B], ob.at[:, pl.ds(0, seqs)])


def solution(mesh):
    n_kv, n_tp = mesh.shape["kv"], mesh.shape["tp"]
    axes = ("kv", "tp")

    def body(tokens, gains, g1, l1, d1, wq, wk, wv, wf, wo, g2, l2, d2, ck, cv, cd):
        seqs, own = tokens.shape
        width = own * n_kv * n_tp
        heads = cd.shape[1]
        groups = heads * HD // LANES
        nz, n_plane = n_kv // NX, NX * n_tp
        arrays = (tokens.T, gains, wq, wk, wv, wf.T, g1.T, l1.T, d1, ck, cd, cv, wo, g2.T, l2.T, d2)
        vm = pltpu.VMEM

        def blocks(*n):
            return vm((*n, TILE, LANES), BF16)

        scratch = [vm(a.shape, a.dtype) for a in arrays] + [
            blocks(n_tp),
            blocks(n_kv),
            vm((ROWS, width), BF16),
            vm((3, NX, LANES, LANES), BF16),
            vm((NX, LANES, LANES), BF16),
            blocks(n_kv),
            blocks(n_kv),
            blocks(n_plane),
            blocks(n_kv),
            blocks(n_kv),
            blocks(n_kv),
            blocks(3),
            blocks(3),
            blocks(nz, 3),
            blocks(nz, 3),
            vm((nz, 3, LANES), F32),
            vm((groups, ROWS, LANES), F32),
            vm((seqs, heads, cd.shape[2]), F32),
            vm((seqs, heads, cd.shape[2]), BF16),
            vm((seqs, heads, LANES), F32),
            vm((seqs * heads, heads * HD), F32),
            blocks(groups),
            vm((groups, 2, LANES), F32),
            blocks(n_kv + 1),
            vm((n_kv + 1, 2, LANES), F32),
            vm((LANES, LANES), F32),
            blocks(NX),
            blocks(n_plane),
            blocks(n_kv),
            vm((n_kv, ROWS, LANES), F32),
            blocks(n_kv),
            blocks(n_kv),
            blocks(n_tp),
            vm((n_kv, 1, LANES), F32),
            pltpu.SemaphoreType.DMA((len(arrays),)),
            pltpu.SemaphoreType.DMA((STAGES,)),
            pltpu.SemaphoreType.DMA((STAGES,)),
            pltpu.SemaphoreType.REGULAR((3,)),
        ]
        out = pl.pallas_call(
            functools.partial(kernel, n_kv, n_tp, seqs, width),
            out_shape=jax.ShapeDtypeStruct((own, seqs), BF16),
            in_specs=[pl.BlockSpec(memory_space=pl.ANY)] * len(arrays),
            out_specs=pl.BlockSpec(memory_space=pltpu.VMEM),
            scratch_shapes=scratch,
            compiler_params=pltpu.CompilerParams(
                collective_id=0, has_side_effects=True, vmem_limit_bytes=56 * 1024 * 1024
            ),
            name="layer",
        )(*arrays)
        return out.T

    placed = (
        P(None, axes), P(), P(None, axes), P(None, axes), P(axes, None), P("kv", "tp"), P("kv", "tp"), P("kv", "tp"),
        P(None, "tp"), P("tp", "kv"), P(None, axes), P(None, axes), P(axes, None), P(None, "kv", "tp"),
        P(None, "kv", "tp"), P(None, "tp", "kv"),
    )
    return jax.shard_map(body, mesh=mesh, in_specs=placed, out_specs=P(None, axes), check_vma=False)
```

```python
import functools

import jax
import jax.numpy as jnp
from jax import lax
from jax.experimental import pallas as pl
from jax.experimental.pallas import tpu as pltpu
from jax.sharding import PartitionSpec as P

MESH = pl.DeviceIdType.MESH
F32, BF16 = jnp.float32, jnp.bfloat16
EPS = 1e-06
HD = 64
LANES = 128
ROWS = 24
TILE = 32
NX = 4
STAGES = 22
(T_TOK, K_TOK, X_Q, X_W, X_WO, R_F1, P_F1, K_QA, K_QB, O_A, O_B, Z_ST, Z_OWN, Z_OWNL, K_B, R_ATT, R_LSE, P_MIX, K_MIX,
 R_F2, T_F2, K_STAT) = range(STAGES)


def nt(a, b):
    return lax.dot_general(a, b, (((1,), (1,)), ((), ())), preferred_element_type=F32)


def nn(a, b):
    return jnp.dot(a, b, preferred_element_type=F32)


def lane_sum(v):
    return jnp.sum(v, axis=-1, keepdims=True)


def rows_of(ref, k):
    return ref[k, 0:ROWS, :].astype(F32)


def put_rows(ref, k, v):
    ref[k, 0:ROWS, :] = v.astype(BF16)


def total_of(buf, slots):
    slots = list(slots)
    return functools.reduce(lambda a, k: a + rows_of(buf, k), slots[1:], rows_of(buf, slots[0]))


def padded(v):
    return jnp.concatenate([v, jnp.zeros((ROWS - v.shape[0], v.shape[1]), v.dtype)], axis=0)


def silu(v):
    return v / (1.0 + jnp.exp(-v))


def kernel(
    n_kv, n_tp, seqs, width,
    tok_h, gains_h, wq_h, wk_h, wv_h, wf_h, g1_h, l1_h, d1_h, ck_h, cd_h, cv_h, wo_h, g2_h, l2_h, d2_h,
    out_ref,
    tok, gains, wk, wv, wf, g1, l1, d1, ck, cd, cv, wo, g2, l2, d2,
    ttok, xb, xn, wqf, wx, wo2, pf, rf, pb, bb, qa, qb, oa, ob, roa, rob, zst, qf, sc, wt, si, om, so, ls, ro, rl, wsq,
    sm, rm, mb, mid, pf2, rf2, tf2, stb,
    load_sem, ssem, rsem, hello,
):
    kv, tp = lax.axis_index("kv"), lax.axis_index("tp")
    nz = n_kv // NX
    zz, xx = kv // NX, kv % NX
    n_plane = NX * n_tp
    me = xx * n_tp + tp
    heads = cd.shape[1]
    groups = heads * HD // LANES
    zwide = NX * LANES
    zcol = pl.multiple_of(zz * zwide, LANES)
    xcol = pl.multiple_of(xx * LANES, LANES)
    col = pl.multiple_of(kv * LANES, LANES)

    loads = [
        pltpu.make_async_copy(h, v, load_sem.at[i])
        for i, (h, v) in enumerate(
            [(tok_h, tok), (gains_h, gains), (wq_h, wqf.at[xx]), (wk_h, wk), (wv_h, wv), (wf_h, wf), (g1_h, g1), (l1_h, l1),
             (d1_h, d1), (ck_h, ck), (cd_h, cd), (cv_h, cv), (wo_h, wo), (g2_h, g2), (l2_h, l2), (d2_h, d2)]
        )
    ]
    for copy in loads:
        copy.start()

    def ordered(i, n):
        return (n // 2 + ((i + 1) // 2) * (1 - 2 * (i % 2)) + n) % n

    def shift(i, d, n):
        return lax.rem(i + d, n)

    def kv_at(dz, dx):
        return shift(zz, dz % nz, nz) * NX + shift(xx, dx, NX)

    x_of = [shift(xx, ordered(i, NX), NX) for i in range(NX)]

    def at(x):
        return zz * NX + x

    def each_kv(visit, same_z=True):
        @pl.loop(0, nz - 1)
        def _(i):
            first = shift(zz, ordered(i, nz), nz) * NX
            for x in x_of:
                visit(first + x, x)

        if same_z:
            for x in x_of[:-1]:
                visit(at(x), x)

    def each_plane(visit):
        @pl.loop(0, n_tp - 1)
        def _(i):
            t = shift(tp, ordered(i, n_tp), n_tp)
            for x in x_of:
                visit(x, t)

        for x in x_of[:-1]:
            visit(x, tp)

    z_own = (2 * xx + tp) % nz
    owns = zz == z_own

    def send(src, dst, stage, **where):
        pltpu.make_async_remote_copy(
            src_ref=src, dst_ref=dst, send_sem=ssem.at[stage], recv_sem=rsem.at[stage],
            device_id=where, device_id_type=MESH,
        ).start()

    def wait(sem, ref):
        pltpu.make_async_copy(ref, ref, sem).wait()

    def part(buf, slot):
        if buf.shape[-2] != TILE:
            return buf.at[slot]
        if len(buf.shape) == 4:
            return buf.at[slot, :, pl.ds(0, seqs)]
        return buf.at[slot, pl.ds(0, seqs)]

    def got(stage, buf, n):
        wait(rsem.at[stage], part(buf, pl.ds(0, n)))

    def gone(stage, buf, n):
        wait(ssem.at[stage], part(buf, pl.ds(0, n)))

    def to_all_kv(buf, stage, same_z=True):
        each_kv(lambda k, x: send(part(buf, kv), part(buf, kv), stage, kv=k), same_z)

    def to_all_tp(buf, stage):
        @pl.loop(0, n_tp - 1)
        def _(i):
            send(part(buf, tp), part(buf, tp), stage, tp=shift(tp, ordered(i, n_tp), n_tp))

    def to_all_z(buf, slot, stage):
        @pl.loop(0, nz - 1)
        def _(i):
            send(part(buf, slot), part(buf, slot), stage, kv=shift(zz, ordered(i, nz), nz) * NX + xx)

    def to_kv_blocks(src, dst, stage):
        each_kv(lambda k, x: send(part(src, k), part(dst, kv), stage, kv=k))
        dst[kv] = src[kv]

    barrier = pltpu.get_barrier_semaphore()
    for i in range(n_tp - 1):
        pl.semaphore_signal(barrier, inc=1, device_id={"tp": shift(tp, i + 1, n_tp)}, device_id_type=MESH)
    for dz, dx in [(0, d) for d in range(1, NX)] + [(1, 0), (-1, 0)]:
        pl.semaphore_signal(barrier, inc=1, device_id={"kv": kv_at(dz, dx)}, device_id_type=MESH)

    loads[0].wait()
    own_w = tok.shape[0]
    lane = lax.broadcasted_iota(jnp.int32, (own_w, LANES), 1)
    row = lax.broadcasted_iota(jnp.int32, (own_w, LANES), 0)
    place = jnp.where(lane == row + own_w * tp, 1.0, 0.0).astype(BF16)
    mine = lax.dot_general(tok[...], place, (((0,), (0,)), ((), ())), preferred_element_type=F32)
    put_rows(ttok, tp, padded(mine))

    pl.semaphore_wait(barrier, n_tp - 1 + NX - 1 + 2)

    def hear(n, step):
        for dz in (step, -step):
            pl.semaphore_signal(hello.at[n], inc=1, device_id={"kv": kv_at(dz, 0)}, device_id_type=MESH)
        if n != 1:
            pl.semaphore_wait(hello.at[n], 2)

    to_all_tp(ttok, T_TOK)
    hear(0, 1)
    hear(1, 2)
    for i in range(3, 5):
        loads[i].wait()
    for d in range(1, NX):
        j = shift(xx, d, NX)
        for m, w in enumerate((wk, wv)):
            send(w.at[:, pl.ds(pl.multiple_of(j * LANES, LANES), LANES)], wx.at[m, xx], X_W, kv=at(j))
    pl.semaphore_wait(hello.at[1], 2)
    hear(2, 1)
    for m, w in enumerate((wk, wv)):
        wx[m, xx] = w[:, pl.ds(xcol, LANES)]
    got(T_TOK, ttok, n_tp - 1)
    put_rows(xb, kv, total_of(ttok, range(n_tp)))
    to_all_kv(xb, K_TOK)
    loads[2].wait()
    for x in x_of[:-1]:
        send(wqf.at[xx], wqf.at[xx], X_Q, kv=at(x))

    def gain(i, k):
        return gains[i : i + 1, k * LANES : (k + 1) * LANES]

    def zgain(i):
        return gains[i : i + 1, pl.ds(zcol, zwide)]

    def feed_forward(gate_w, lift_w, down_w, part_out):
        x = xn[...]
        act = (silu(nt(x, gate_w[...])) * nt(x, lift_w[...])).astype(BF16)
        for c in range(0, n_kv, 4):
            some = nn(act, down_w[:, c * LANES : (c + 4) * LANES])
            for j in range(4):
                put_rows(part_out, c + j, some[:, j * LANES : (j + 1) * LANES])

    lane_r = lax.broadcasted_iota(jnp.int32, (ROWS, LANES), 1)
    low = lane_r < HD
    eye = lax.broadcasted_iota(jnp.int32, (ROWS, LANES), 0) == lane_r

    def flat(column):
        return jnp.sum(jnp.where(eye, column, 0.0), axis=0, keepdims=True)

    def upright(line):
        return lane_sum(jnp.where(eye, jnp.broadcast_to(line, (ROWS, LANES)), 0.0))

    loads[1].wait()
    got(K_TOK, xb, n_kv - 1)
    squares = jnp.zeros((ROWS, LANES), F32)
    for k in range(n_kv):
        v = rows_of(xb, k)
        squares = squares + v * v
    s_tt = lane_sum(squares)
    scale = lax.rsqrt(s_tt / width + EPS)
    for k in range(n_kv):
        xn[:, k * LANES : (k + 1) * LANES] = (rows_of(xb, k) * scale * gain(0, k)).astype(BF16)
    for i in range(6, 9):
        loads[i].wait()
    feed_forward(g1, l1, d1, pf)
    to_kv_blocks(pf, rf, R_F1)

    loads[5].wait()
    wait(rsem.at[X_W], wx.at[:, pl.ds(0, NX - 1)])
    got(X_Q, wqf, NX - 1)
    tz = jnp.concatenate([rows_of(xb, at(x)) for x in range(NX)], axis=1)
    lane_f = lax.broadcasted_iota(jnp.int32, (ROWS, heads), 1)

    def projections(x, q_out, o_out):
        q = nn(x, wqf[...].reshape(zwide, groups * LANES))
        k, v = [nn(x, wx[m].reshape(zwide, LANES)) for m in range(2)]
        f = nt(x, wf[:, pl.ds(zcol, zwide)])
        f0, f1 = [lane_sum(jnp.where(lane_f == 2 * xx + g, f, 0.0)) for g in range(2)]
        for j in range(groups):
            q_out[zz, j, 0:ROWS, :] = q[:, j * LANES : (j + 1) * LANES].astype(BF16)
        put_rows(o_out, 0, k)
        put_rows(o_out, 1, v)
        put_rows(o_out, 2, jnp.where(low, f0, f1))

    def to_owner(src, dst, stage):
        whole = src.at[:, pl.ds(0, seqs)]

        @pl.when(jnp.logical_not(owns))
        def _():
            send(whole, dst.at[zz, :, pl.ds(0, seqs)], stage, kv=z_own * NX + xx)

        @pl.when(owns)
        def _():
            dst[zz] = src[...]

    projections((tz * zgain(2)).astype(BF16), qa, oa)

    got(R_F1, rf, n_kv - 1)
    put_rows(pb, me, total_of(rf, range(n_kv)))

    def to_plane(src, dst, stage, pick):
        each_plane(lambda x, t: send(part(src, pick(x)), part(dst, me), stage, kv=at(x), tp=t))

    to_plane(pb, pb, P_F1, lambda x: me)
    to_all_z(qa, zz, K_QA)
    to_owner(oa, roa, O_A)

    got(P_F1, pb, n_plane - 1)
    for x in range(NX):
        put_rows(bb, at(x), total_of(pb, range(x * n_tp, (x + 1) * n_tp)))
    bz = jnp.concatenate([rows_of(bb, at(x)) for x in range(NX)], axis=1)
    u = bz * zgain(1)
    projections((u * zgain(2)).astype(BF16), qb, ob)
    to_all_z(qb, zz, K_QB)
    for n, stat in enumerate((bz * bz, tz * u, u * u)):
        zst[zz, n : n + 1, :] = flat(lane_sum(stat))
    to_all_z(zst, zz, Z_ST)
    to_owner(ob, rob, O_B)

    got(K_QA, qa, nz - 1)
    got(Z_ST, zst, nz - 1)
    stats = functools.reduce(lambda a, z: a + zst[z], range(1, nz), zst[0])
    s_bb, s_tu, s_uu = [upright(stats[n : n + 1]) for n in range(3)]
    r1 = lax.rsqrt(s_bb / width + EPS)
    half = 0.5 * r1
    scale_mid = lax.rsqrt((s_tt + r1 * s_tu + half * half * s_uu) / width + EPS)
    got(K_QB, qb, nz - 1)
    for j in range(groups):
        a, b = [functools.reduce(lambda t, more: t + more, [p[z, j, 0:ROWS, :].astype(F32) for z in range(nz)]) for p in (qa, qb)]
        qf[j] = (scale_mid * (a + half * b)).astype(BF16).astype(F32)

    loads[12].wait()
    for d in range(1, NX):
        j = shift(xx, d, NX)
        send(wo.at[pl.ds(pl.multiple_of(j * LANES, LANES), LANES), :], wo2.at[xx], X_WO, kv=at(j))
    wo2[xx] = wo[pl.ds(xcol, LANES), :]
    for i in range(9, 12):
        loads[i].wait()
    head_i = lax.broadcasted_iota(jnp.int32, (heads, LANES), 0)
    lane_h = lax.broadcasted_iota(jnp.int32, (heads, LANES), 1)
    masks = [head_i == 2 * j + lane_h // HD for j in range(groups)]
    batch = 18

    @pl.loop(0, seqs, step=batch)
    def _(first):
        for i in range(batch):
            b = first + i
            rows = [
                jnp.where(masks[j], jnp.broadcast_to(qf[j, pl.ds(b, 1), :], (heads, LANES)), 0.0) for j in range(groups)
            ]
            query = jnp.concatenate(rows, axis=1).astype(BF16)
            sc[b] = nt(query, ck[b]) * (HD**-0.5) + cd[b]

    score = sc[...]
    peak = jnp.max(score, axis=2, keepdims=True)
    raised = jnp.exp(score - peak)
    total = jnp.sum(raised, axis=2, keepdims=True)
    wt[...] = raised.astype(BF16)
    si[...] = jnp.broadcast_to(1.0 / total, (seqs, heads, LANES))
    level = jnp.broadcast_to(peak + jnp.log(total), (seqs, heads, LANES))
    turn = lax.broadcasted_iota(jnp.int32, (seqs, heads, LANES), 0) == lax.broadcasted_iota(
        jnp.int32, (seqs, heads, LANES), 2
    )
    lines = jnp.sum(jnp.where(turn, level, 0.0), axis=0)
    for j in range(groups):
        ls[j] = lines[2 * j : 2 * j + 2]

    @pl.loop(0, seqs, step=batch)
    def _(first):
        for i in range(batch):
            b = first + i
            o = nn(wt[b], cv[b])
            share = si[b]
            here = pl.ds(pl.multiple_of(b * heads, heads), heads)
            for j in range(groups):
                om[here, j * LANES : (j + 1) * LANES] = jnp.where(masks[j], o[:, j * LANES : (j + 1) * LANES] * share, 0.0)

    pick = lax.broadcasted_iota(jnp.int32, (ROWS, seqs * heads), 1) // heads
    pick = jnp.where(pick == lax.broadcasted_iota(jnp.int32, (ROWS, seqs * heads), 0), 1.0, 0.0).astype(BF16)
    outs = nn(pick, om[...].astype(BF16))
    for j in range(groups):
        put_rows(so, j, outs[:, j * LANES : (j + 1) * LANES])

    def deliver(k, x):
        send(ls.at[x], rl.at[kv], R_LSE, kv=k)
        send(part(so, x), part(ro, kv), R_ATT, kv=k)

    each_kv(deliver)
    ro[kv] = so[xx]
    rl[kv] = ls[xx]

    @pl.when(owns)
    def _():
        got(O_A, roa, nz - 1)
        got(O_B, rob, nz - 1)

        def finished(n):
            a = functools.reduce(lambda t, z: t + roa[z, n, 0:ROWS, :].astype(F32), range(1, nz), roa[0, n, 0:ROWS, :].astype(F32))
            b = functools.reduce(lambda t, z: t + rob[z, n, 0:ROWS, :].astype(F32), range(1, nz), rob[0, n, 0:ROWS, :].astype(F32))
            return scale_mid * (a + half * b)

        k, v, f = [finished(n) for n in range(3)]
        qk = qf[xx] * k.astype(BF16).astype(F32)
        forget = jnp.minimum(f, 0.0) - jnp.log(1.0 + jnp.exp(-jnp.abs(f)))
        own0 = lane_sum(jnp.where(low, qk, 0.0)) * (HD**-0.5) - forget[:, 0:1]
        own1 = lane_sum(jnp.where(low, 0.0, qk)) * (HD**-0.5) - forget[:, HD : HD + 1]
        put_rows(ro, n_kv, v)
        rl[n_kv, 0:1, :] = flat(own0)
        rl[n_kv, 1:2, :] = flat(own1)
        to_all_z(rl, n_kv, Z_OWNL)
        to_all_z(ro, n_kv, Z_OWN)

    @pl.when(jnp.logical_not(owns))
    def _():
        wait(rsem.at[Z_OWNL], rl.at[n_kv])
        wait(rsem.at[Z_OWN], part(ro, n_kv))

    got(R_LSE, rl, n_kv - 1)
    n_src = n_kv + 1
    top = functools.reduce(jnp.maximum, [rl[s] for s in range(n_src)])
    raised = [jnp.exp(rl[s] - top) for s in range(n_src)]
    norm = 1.0 / functools.reduce(lambda a, b: a + b, raised)
    for s in range(n_src):
        wsq[2 * s : 2 * s + 2, :] = raised[s] * norm
    weights = wsq[...].T[0:ROWS]
    got(R_ATT, ro, n_kv - 1)
    joined = jnp.zeros((ROWS, LANES), F32)
    for s in range(n_src):
        joined = joined + jnp.where(low, weights[:, 2 * s : 2 * s + 1], weights[:, 2 * s + 1 : 2 * s + 2]) * rows_of(ro, s)
    attended = joined.astype(BF16)
    wait(rsem.at[X_WO], wo2.at[pl.ds(0, NX - 1)])
    for x in range(NX):
        put_rows(sm, x, nn(attended, wo2[x]))

    to_plane(sm, rm, P_MIX, lambda x: x)
    rm[me] = sm[xx]
    to_all_kv(bb, K_B, False)
    got(P_MIX, rm, n_plane - 1)
    put_rows(mb, kv, total_of(rm, range(n_plane)))

    to_all_kv(mb, K_MIX)
    for i in range(13, 16):
        loads[i].wait()

    got(K_B, bb, n_kv - NX)
    for k in range(n_kv):
        mid[k] = rows_of(xb, k) + rows_of(bb, k) * half * gain(1, k)

    got(K_MIX, mb, n_kv - 1)

    squares = jnp.zeros((ROWS, LANES), F32)
    for k in range(n_kv):
        v = rows_of(mb, k)
        squares = squares + v * v
    scale = lax.rsqrt(lane_sum(squares) / width + EPS)
    squares = jnp.zeros((ROWS, LANES), F32)
    for k in range(n_kv):
        v = mid[k] + rows_of(mb, k) * scale * gain(3, k)
        mid[k] = v
        squares = squares + v * v
    scale = lax.rsqrt(lane_sum(squares) / width + EPS)
    for k in range(n_kv):
        xn[:, k * LANES : (k + 1) * LANES] = (mid[k] * scale * gain(4, k)).astype(BF16)
    feed_forward(g2, l2, d2, pf2)
    to_kv_blocks(pf2, rf2, R_F2)
    got(R_F2, rf2, n_kv - 1)
    put_rows(tf2, tp, total_of(rf2, range(n_kv)))
    to_all_tp(tf2, T_F2)
    got(T_F2, tf2, n_tp - 1)
    bf = total_of(tf2, range(n_tp))

    stb[kv] = flat(lane_sum(bf * bf))
    to_all_kv(stb, K_STAT)
    got(K_STAT, stb, n_kv - 1)
    line = functools.reduce(lambda a, k: a + stb[k], range(1, n_kv), stb[0])
    scale = lax.rsqrt(upright(line) / width + EPS)
    final = (mid[kv] + 0.5 * (bf * scale * gains[5:6, pl.ds(col, LANES)])).astype(BF16)
    out_ref[...] = nt(place, final)[:, 0:seqs].astype(BF16)

    for stage, buf, n in (
        (T_TOK, ttok, n_tp - 1), (T_F2, tf2, n_tp - 1), (K_TOK, xb, n_kv - 1), (R_F1, pf, n_kv - 1), (P_F1, pb, n_plane - 1),
        (K_QA, qa, nz - 1), (K_QB, qb, nz - 1), (X_Q, wqf, NX - 1), (Z_ST, zst, nz - 1), (K_B, bb, n_kv - NX), (R_ATT, ro, n_kv - 1),
        (R_LSE, rl, n_kv - 1), (P_MIX, rm, n_plane - 1), (K_MIX, mb, n_kv - 1), (R_F2, pf2, n_kv - 1), (K_STAT, stb, n_kv - 1),
    ):
        gone(stage, buf, n)
    wait(ssem.at[X_W], wx.at[:, pl.ds(0, NX - 1)])
    wait(ssem.at[X_WO], wo2.at[pl.ds(0, NX - 1)])

    @pl.when(owns)
    def _():
        gone(Z_OWNL, rl, nz - 1)
        gone(Z_OWN, ro, nz - 1)

    @pl.when(jnp.logical_not(owns))
    def _():
        wait(ssem.at[O_A], oa.at[:, pl.ds(0, seqs)])
        wait(ssem.at[O_B], ob.at[:, pl.ds(0, seqs)])


def solution(mesh):
    n_kv, n_tp = mesh.shape["kv"], mesh.shape["tp"]
    axes = ("kv", "tp")

    def body(tokens, gains, g1, l1, d1, wq, wk, wv, wf, wo, g2, l2, d2, ck, cv, cd):
        seqs, own = tokens.shape
        width = own * n_kv * n_tp
        heads = cd.shape[1]
        groups = heads * HD // LANES
        nz, n_plane = n_kv // NX, NX * n_tp
        arrays = (tokens.T, gains, wq, wk, wv, wf.T, g1.T, l1.T, d1, ck, cd, cv, wo, g2.T, l2.T, d2)
        arrays = tuple(pltpu.with_memory_space_constraint(a, pltpu.HBM) for a in arrays)
        vm = pltpu.VMEM

        def blocks(*n):
            return vm((*n, TILE, LANES), BF16)

        scratch = [vm(a.shape, a.dtype) for i, a in enumerate(arrays) if i != 2] + [
            blocks(n_tp),
            blocks(n_kv),
            vm((ROWS, width), BF16),
            vm((NX, LANES, groups * LANES), BF16),
            vm((2, NX, LANES, LANES), BF16),
            vm((NX, LANES, LANES), BF16),
            blocks(n_kv),
            blocks(n_kv),
            blocks(n_plane),
            blocks(n_kv),
            blocks(nz, groups),
            blocks(nz, groups),
            blocks(3),
            blocks(3),
            blocks(nz, 3),
            blocks(nz, 3),
            vm((nz, 3, LANES), F32),
            vm((groups, ROWS, LANES), F32),
            vm((seqs, heads, cd.shape[2]), F32),
            vm((seqs, heads, cd.shape[2]), BF16),
            vm((seqs, heads, LANES), F32),
            vm((seqs * heads, heads * HD), F32),
            blocks(groups),
            vm((groups, 2, LANES), F32),
            blocks(n_kv + 1),
            vm((n_kv + 1, 2, LANES), F32),
            vm((LANES, LANES), F32),
            blocks(NX),
            blocks(n_plane),
            blocks(n_kv),
            vm((n_kv, ROWS, LANES), F32),
            blocks(n_kv),
            blocks(n_kv),
            blocks(n_tp),
            vm((n_kv, 1, LANES), F32),
            pltpu.SemaphoreType.DMA((len(arrays),)),
            pltpu.SemaphoreType.DMA((STAGES,)),
            pltpu.SemaphoreType.DMA((STAGES,)),
            pltpu.SemaphoreType.REGULAR((3,)),
        ]
        out = pl.pallas_call(
            functools.partial(kernel, n_kv, n_tp, seqs, width),
            out_shape=jax.ShapeDtypeStruct((own, seqs), BF16),
            in_specs=[pl.BlockSpec(memory_space=pl.ANY)] * len(arrays),
            out_specs=pl.BlockSpec(memory_space=pltpu.VMEM),
            scratch_shapes=scratch,
            compiler_params=pltpu.CompilerParams(
                collective_id=0, has_side_effects=True, vmem_limit_bytes=26 * 1024 * 1024
            ),
            name="layer",
        )(*arrays)
        return out.T

    placed = (
        P(None, axes), P(), P(None, axes), P(None, axes), P(axes, None), P("kv", "tp"), P("kv", "tp"), P("kv", "tp"),
        P(None, "tp"), P("tp", "kv"), P(None, axes), P(None, axes), P(axes, None), P(None, "kv", "tp"),
        P(None, "kv", "tp"), P(None, "tp", "kv"),
    )
    return jax.shard_map(body, mesh=mesh, in_specs=placed, out_specs=P(None, axes), check_vma=False)
```

```python
import functools

import jax
import jax.numpy as jnp
from jax import lax
from jax.experimental import pallas as pl
from jax.experimental.pallas import tpu as pltpu
from jax.sharding import PartitionSpec as P

MESH = pl.DeviceIdType.MESH
F32, BF16 = jnp.float32, jnp.bfloat16
EPS = 1e-06
HD = 64
LANES = 128
ROWS = 24
TILE = 32
NX = 4
STAGES = 22
(T_TOK, K_TOK, X_Q, X_W, X_WO, R_F1, P_F1, K_QA, K_QB, O_A, O_B, Z_ST, Z_OWN, Z_OWNL, K_B, R_ATT, R_LSE, P_MIX, K_MIX,
 R_F2, T_F2, K_STAT) = range(STAGES)


def nt(a, b):
    return lax.dot_general(a, b, (((1,), (1,)), ((), ())), preferred_element_type=F32)


def nn(a, b):
    return jnp.dot(a, b, preferred_element_type=F32)


def lane_sum(v):
    return jnp.sum(v, axis=-1, keepdims=True)


def rows_of(ref, k):
    return ref[k, 0:ROWS, :].astype(F32)


def put_rows(ref, k, v):
    ref[k, 0:ROWS, :] = v.astype(BF16)


def total_of(buf, slots):
    slots = list(slots)
    return functools.reduce(lambda a, k: a + rows_of(buf, k), slots[1:], rows_of(buf, slots[0]))


def padded(v):
    return jnp.concatenate([v, jnp.zeros((ROWS - v.shape[0], v.shape[1]), v.dtype)], axis=0)


def silu(v):
    return v / (1.0 + jnp.exp(-v))


def kernel(
    n_kv, n_tp, seqs, width,
    tok_h, gains_h, wq_h, wk_h, wv_h, wf_h, g1_h, l1_h, d1_h, ck_h, cd_h, cv_h, wo_h, g2_h, l2_h, d2_h,
    out_ref,
    tok, gains, wk, wv, wf, g1, l1, d1, ck, cd, cv, wo, g2, l2, d2,
    ckt, ttok, xb, wqf, wx, wo2, pf, rf, pb, bb, qa, qb, oa, ob, roa, rob, zst, qf, sc, wt, si, om, so, ls, ro, rl, wsq, wexp,
    sm, rm, mb, mid, pf2, rf2, tf2, stb,
    load_sem, ssem, rsem, hello,
):
    kv, tp = lax.axis_index("kv"), lax.axis_index("tp")
    nz = n_kv // NX
    zz, xx = kv // NX, kv % NX
    n_plane = NX * n_tp
    me = xx * n_tp + tp
    heads = cd.shape[1]
    groups = heads * HD // LANES
    zwide = NX * LANES
    zcol = pl.multiple_of(zz * zwide, LANES)
    xcol = pl.multiple_of(xx * LANES, LANES)
    col = pl.multiple_of(kv * LANES, LANES)

    loads = [
        pltpu.make_async_copy(h, v, load_sem.at[i])
        for i, (h, v) in enumerate(
            [(tok_h, tok), (gains_h, gains), (wq_h, wqf.at[xx]), (wk_h, wk), (wv_h, wv), (wf_h, wf), (g1_h, g1), (l1_h, l1),
             (d1_h, d1), (ck_h, ck), (cd_h, cd), (cv_h, cv), (wo_h, wo), (g2_h, g2), (l2_h, l2), (d2_h, d2)]
        )
    ]
    for copy in loads:
        copy.start()

    def ordered(i, n):
        return (n // 2 + ((i + 1) // 2) * (1 - 2 * (i % 2)) + n) % n

    def shift(i, d, n):
        return lax.rem(i + d, n)

    def kv_at(dz, dx):
        return shift(zz, dz % nz, nz) * NX + shift(xx, dx, NX)

    x_of = [shift(xx, ordered(i, NX), NX) for i in range(NX)]

    def at(x):
        return zz * NX + x

    def each_kv(visit, same_z=True):
        @pl.loop(0, nz - 1)
        def _(i):
            first = shift(zz, ordered(i, nz), nz) * NX
            for x in x_of:
                visit(first + x, x)

        if same_z:
            for x in x_of[:-1]:
                visit(at(x), x)

    def each_plane(visit):
        @pl.loop(0, n_tp - 1)
        def _(i):
            t = shift(tp, ordered(i, n_tp), n_tp)
            for x in x_of:
                visit(x, t)

        for x in x_of[:-1]:
            visit(x, tp)

    z_own = (2 * xx + tp) % nz
    owns = zz == z_own

    def send(src, dst, stage, **where):
        pltpu.make_async_remote_copy(
            src_ref=src, dst_ref=dst, send_sem=ssem.at[stage], recv_sem=rsem.at[stage],
            device_id=where, device_id_type=MESH,
        ).start()

    def wait(sem, ref):
        pltpu.make_async_copy(ref, ref, sem).wait()

    def part(buf, slot):
        if buf.shape[-2] != TILE:
            return buf.at[slot]
        if len(buf.shape) == 4:
            return buf.at[slot, :, pl.ds(0, seqs)]
        return buf.at[slot, pl.ds(0, seqs)]

    def got(stage, buf, n):
        wait(rsem.at[stage], part(buf, pl.ds(0, n)))

    def gone(stage, buf, n):
        wait(ssem.at[stage], part(buf, pl.ds(0, n)))

    def to_all_kv(buf, stage, same_z=True):
        each_kv(lambda k, x: send(part(buf, kv), part(buf, kv), stage, kv=k), same_z)

    def to_all_tp(buf, stage):
        @pl.loop(0, n_tp - 1)
        def _(i):
            send(part(buf, tp), part(buf, tp), stage, tp=shift(tp, ordered(i, n_tp), n_tp))

    def to_all_z(buf, slot, stage):
        @pl.loop(0, nz - 1)
        def _(i):
            send(part(buf, slot), part(buf, slot), stage, kv=shift(zz, ordered(i, nz), nz) * NX + xx)

    def to_kv_blocks(src, dst, stage):
        each_kv(lambda k, x: send(part(src, k), part(dst, kv), stage, kv=k))
        dst[kv] = src[kv]

    barrier = pltpu.get_barrier_semaphore()
    for i in range(n_tp - 1):
        pl.semaphore_signal(barrier, inc=1, device_id={"tp": shift(tp, i + 1, n_tp)}, device_id_type=MESH)
    for dz, dx in [(0, d) for d in range(1, NX)] + [(1, 0), (-1, 0)]:
        pl.semaphore_signal(barrier, inc=1, device_id={"kv": kv_at(dz, dx)}, device_id_type=MESH)

    loads[0].wait()
    own_w = tok.shape[0]
    lane = lax.broadcasted_iota(jnp.int32, (own_w, LANES), 1)
    row = lax.broadcasted_iota(jnp.int32, (own_w, LANES), 0)
    place = jnp.where(lane == row + own_w * tp, 1.0, 0.0).astype(BF16)
    mine = lax.dot_general(tok[...], place, (((0,), (0,)), ((), ())), preferred_element_type=F32)
    put_rows(ttok, tp, padded(mine))

    pl.semaphore_wait(barrier, n_tp - 1 + NX - 1 + 2)

    def hear(n, step):
        for dz in (step, -step):
            pl.semaphore_signal(hello.at[n], inc=1, device_id={"kv": kv_at(dz, 0)}, device_id_type=MESH)
        if n != 1:
            pl.semaphore_wait(hello.at[n], 2)

    to_all_tp(ttok, T_TOK)
    hear(0, 1)
    hear(1, 2)
    for i in range(3, 5):
        loads[i].wait()
    for d in range(1, NX):
        j = shift(xx, d, NX)
        for m, w in enumerate((wk, wv)):
            send(w.at[:, pl.ds(pl.multiple_of(j * LANES, LANES), LANES)], wx.at[m, xx], X_W, kv=at(j))
    pl.semaphore_wait(hello.at[1], 2)
    hear(2, 1)
    for m, w in enumerate((wk, wv)):
        wx[m, xx] = w[:, pl.ds(xcol, LANES)]
    got(T_TOK, ttok, n_tp - 1)
    put_rows(xb, kv, total_of(ttok, range(n_tp)))
    to_all_kv(xb, K_TOK)
    loads[2].wait()
    for x in x_of[:-1]:
        send(wqf.at[xx], wqf.at[xx], X_Q, kv=at(x))

    def gain(i, k):
        return gains[i : i + 1, k * LANES : (k + 1) * LANES]

    def zgain(i):
        return gains[i : i + 1, pl.ds(zcol, zwide)]

    def products(block, gain_row, gate_w, lift_w):
        squares, gate, lift = [jnp.zeros((ROWS, n), F32) for n in (LANES, gate_w.shape[0], lift_w.shape[0])]
        for c in range(0, n_kv, 4):
            xs = []
            for k in range(c, c + 4):
                v = block(k)
                squares = squares + v * v
                xs.append((v * gain(gain_row, k)).astype(BF16))
            x = jnp.concatenate(xs, axis=1)
            here = slice(c * LANES, (c + 4) * LANES)
            gate = gate + nt(x, gate_w[:, here])
            lift = lift + nt(x, lift_w[:, here])
        return lane_sum(squares), gate, lift

    def feed_forward(scale, gate, lift, down_w, part_out):
        act = (silu(gate * scale) * (lift * scale)).astype(BF16)
        for c in range(0, n_kv, 4):
            some = nn(act, down_w[:, c * LANES : (c + 4) * LANES])
            for j in range(4):
                put_rows(part_out, c + j, some[:, j * LANES : (j + 1) * LANES])

    lane_r = lax.broadcasted_iota(jnp.int32, (ROWS, LANES), 1)
    low = lane_r < HD
    eye = lax.broadcasted_iota(jnp.int32, (ROWS, LANES), 0) == lane_r

    def flat(column):
        return jnp.sum(jnp.where(eye, column, 0.0), axis=0, keepdims=True)

    def upright(line):
        return lane_sum(jnp.where(eye, jnp.broadcast_to(line, (ROWS, LANES)), 0.0))

    loads[1].wait()
    got(K_TOK, xb, n_kv - 1)
    for i in range(6, 9):
        loads[i].wait()
    s_tt, gate, lift = products(lambda k: rows_of(xb, k), 0, g1, l1)
    feed_forward(lax.rsqrt(s_tt / width + EPS), gate, lift, d1, pf)
    to_kv_blocks(pf, rf, R_F1)

    loads[9].wait()

    @pl.loop(0, seqs)
    def _(b):
        ckt[b] = ck[b].T

    loads[5].wait()
    wait(rsem.at[X_W], wx.at[:, pl.ds(0, NX - 1)])
    got(X_Q, wqf, NX - 1)
    tz = jnp.concatenate([rows_of(xb, at(x)) for x in range(NX)], axis=1)
    lane_f = lax.broadcasted_iota(jnp.int32, (ROWS, heads), 1)

    def query_part(x, q_out):
        q = nn(x, wqf[...].reshape(zwide, groups * LANES))
        for j in range(groups):
            q_out[zz, j, 0:ROWS, :] = q[:, j * LANES : (j + 1) * LANES].astype(BF16)

    def other_parts(x, o_out):
        for m in range(2):
            put_rows(o_out, m, nn(x, wx[m].reshape(zwide, LANES)))
        f = nt(x, wf[:, pl.ds(zcol, zwide)])
        f0, f1 = [lane_sum(jnp.where(lane_f == 2 * xx + g, f, 0.0)) for g in range(2)]
        put_rows(o_out, 2, jnp.where(low, f0, f1))

    def to_owner(src, dst, stage):
        whole = src.at[:, pl.ds(0, seqs)]

        @pl.when(jnp.logical_not(owns))
        def _():
            send(whole, dst.at[zz, :, pl.ds(0, seqs)], stage, kv=z_own * NX + xx)

        @pl.when(owns)
        def _():
            dst[zz] = src[...]

    shared = (tz * zgain(2)).astype(BF16)
    query_part(shared, qa)
    other_parts(shared, oa)

    got(R_F1, rf, n_kv - 1)
    put_rows(pb, me, total_of(rf, range(n_kv)))

    def to_plane(src, dst, stage, pick):
        each_plane(lambda x, t: send(part(src, pick(x)), part(dst, me), stage, kv=at(x), tp=t))

    to_plane(pb, pb, P_F1, lambda x: me)
    to_all_z(qa, zz, K_QA)
    to_owner(oa, roa, O_A)

    got(P_F1, pb, n_plane - 1)
    for x in range(NX):
        put_rows(bb, at(x), total_of(pb, range(x * n_tp, (x + 1) * n_tp)))
    bz = jnp.concatenate([rows_of(bb, at(x)) for x in range(NX)], axis=1)
    u = bz * zgain(1)
    shared = (u * zgain(2)).astype(BF16)
    query_part(shared, qb)
    to_all_z(qb, zz, K_QB)
    for n, stat in enumerate((bz * bz, tz * u, u * u)):
        zst[zz, n : n + 1, :] = flat(lane_sum(stat))
    to_all_z(zst, zz, Z_ST)
    other_parts(shared, ob)
    to_owner(ob, rob, O_B)

    got(K_QA, qa, nz - 1)
    got(Z_ST, zst, nz - 1)
    stats = functools.reduce(lambda a, z: a + zst[z], range(1, nz), zst[0])
    s_bb, s_tu, s_uu = [upright(stats[n : n + 1]) for n in range(3)]
    r1 = lax.rsqrt(s_bb / width + EPS)
    half = 0.5 * r1
    scale_mid = lax.rsqrt((s_tt + r1 * s_tu + half * half * s_uu) / width + EPS)

    def z_sum(buf, j):
        return functools.reduce(lambda a, b: a + b, [buf[z, j, 0:ROWS, :].astype(F32) for z in range(nz)])

    from_tokens = [z_sum(qa, j) for j in range(groups)]
    got(K_QB, qb, nz - 1)
    for j in range(groups):
        qf[j] = (scale_mid * (from_tokens[j] + half * z_sum(qb, j))).astype(BF16).astype(F32)

    loads[12].wait()
    for d in range(1, NX):
        j = shift(xx, d, NX)
        send(wo.at[pl.ds(pl.multiple_of(j * LANES, LANES), LANES), :], wo2.at[xx], X_WO, kv=at(j))
    wo2[xx] = wo[pl.ds(xcol, LANES), :]
    for i in range(10, 12):
        loads[i].wait()
    head_i = lax.broadcasted_iota(jnp.int32, (heads, LANES), 0)
    lane_h = lax.broadcasted_iota(jnp.int32, (heads, LANES), 1)
    masks = [head_i == 2 * j + lane_h // HD for j in range(groups)]
    for b in range(seqs):
        rows = [jnp.where(masks[j], jnp.broadcast_to(qf[j, b : b + 1, :], (heads, LANES)), 0.0) for j in range(groups)]
        query = jnp.concatenate(rows, axis=1).astype(BF16)
        sc[b] = nn(query, ckt[b]) * (HD**-0.5) + cd[b]

    score = sc[...]
    peak = jnp.max(score, axis=2, keepdims=True)
    raised = jnp.exp(score - peak)
    total = jnp.sum(raised, axis=2, keepdims=True)
    wt[...] = raised.astype(BF16)
    si[...] = jnp.broadcast_to(1.0 / total, (seqs, heads, LANES))
    level = jnp.broadcast_to(peak + jnp.log(total), (seqs, heads, LANES))
    turn = lax.broadcasted_iota(jnp.int32, (seqs, heads, LANES), 0) == lax.broadcasted_iota(
        jnp.int32, (seqs, heads, LANES), 2
    )
    lines = jnp.sum(jnp.where(turn, level, 0.0), axis=0)
    for j in range(groups):
        ls[j] = lines[2 * j : 2 * j + 2]

    for i in range(n_kv - 1):
        first, x = shift(zz, ordered(i // NX, nz), nz) * NX, x_of[i % NX]
        send(ls.at[x], rl.at[kv], R_LSE, kv=first + x)
    rl[kv] = ls[xx]

    for b in range(seqs):
        o = nn(wt[b], cv[b])
        share = si[b]
        for j in range(groups):
            om[b * heads : (b + 1) * heads, j * LANES : (j + 1) * LANES] = jnp.where(
                masks[j], o[:, j * LANES : (j + 1) * LANES] * share, 0.0
            )

    pick = lax.broadcasted_iota(jnp.int32, (ROWS, seqs * heads), 1) // heads
    pick = jnp.where(pick == lax.broadcasted_iota(jnp.int32, (ROWS, seqs * heads), 0), 1.0, 0.0).astype(BF16)
    outs = nn(pick, om[...].astype(BF16))
    for j in range(groups):
        put_rows(so, j, outs[:, j * LANES : (j + 1) * LANES])

    each_kv(lambda k, x: send(part(so, x), part(ro, kv), R_ATT, kv=k))
    ro[kv] = so[xx]

    @pl.when(owns)
    def _():
        got(O_A, roa, nz - 1)
        got(O_B, rob, nz - 1)

        def finished(n):
            a = functools.reduce(lambda t, z: t + roa[z, n, 0:ROWS, :].astype(F32), range(1, nz), roa[0, n, 0:ROWS, :].astype(F32))
            b = functools.reduce(lambda t, z: t + rob[z, n, 0:ROWS, :].astype(F32), range(1, nz), rob[0, n, 0:ROWS, :].astype(F32))
            return scale_mid * (a + half * b)

        k, v, f = [finished(n) for n in range(3)]
        qk = qf[xx] * k.astype(BF16).astype(F32)
        forget = jnp.minimum(f, 0.0) - jnp.log(1.0 + jnp.exp(-jnp.abs(f)))
        own0 = lane_sum(jnp.where(low, qk, 0.0)) * (HD**-0.5) - forget[:, 0:1]
        own1 = lane_sum(jnp.where(low, 0.0, qk)) * (HD**-0.5) - forget[:, HD : HD + 1]
        put_rows(ro, n_kv, v)
        rl[n_kv, 0:1, :] = flat(own0)
        rl[n_kv, 1:2, :] = flat(own1)
        to_all_z(rl, n_kv, Z_OWNL)
        to_all_z(ro, n_kv, Z_OWN)

    @pl.when(jnp.logical_not(owns))
    def _():
        wait(rsem.at[Z_OWNL], rl.at[n_kv])

    got(R_LSE, rl, n_kv - 1)
    n_src = n_kv + 1
    top = functools.reduce(jnp.maximum, [rl[s] for s in range(n_src)])
    raised = [jnp.exp(rl[s] - top) for s in range(n_src)]
    norm = 1.0 / functools.reduce(lambda a, b: a + b, raised)
    for s in range(n_src):
        wsq[2 * s : 2 * s + 2, :] = raised[s] * norm
    weights = wsq[...].T[0:ROWS]
    for s in range(n_src):
        wexp[s] = jnp.where(low, weights[:, 2 * s : 2 * s + 1], weights[:, 2 * s + 1 : 2 * s + 2])

    @pl.when(jnp.logical_not(owns))
    def _():
        wait(rsem.at[Z_OWN], part(ro, n_kv))

    got(R_ATT, ro, n_kv - 1)
    joined = jnp.zeros((ROWS, LANES), F32)
    for s in range(n_src):
        joined = joined + wexp[s] * rows_of(ro, s)
    attended = joined.astype(BF16)
    wait(rsem.at[X_WO], wo2.at[pl.ds(0, NX - 1)])
    for x in range(NX):
        put_rows(sm, x, nn(attended, wo2[x]))

    to_plane(sm, rm, P_MIX, lambda x: x)
    rm[me] = sm[xx]
    to_all_kv(bb, K_B, False)
    got(P_MIX, rm, n_plane - 1)
    put_rows(mb, kv, total_of(rm, range(n_plane)))

    to_all_kv(mb, K_MIX)
    for i in range(13, 16):
        loads[i].wait()

    got(K_B, bb, n_kv - NX)
    for k in range(n_kv):
        mid[k] = rows_of(xb, k) + rows_of(bb, k) * half * gain(1, k)

    got(K_MIX, mb, n_kv - 1)

    squares = jnp.zeros((ROWS, LANES), F32)
    for k in range(n_kv):
        v = rows_of(mb, k)
        squares = squares + v * v
    scale = lax.rsqrt(lane_sum(squares) / width + EPS)

    def after(k):
        mid[k] = mid[k] + rows_of(mb, k) * scale * gain(3, k)
        return mid[k]

    s_aa, gate, lift = products(after, 4, g2, l2)
    feed_forward(lax.rsqrt(s_aa / width + EPS), gate, lift, d2, pf2)
    to_kv_blocks(pf2, rf2, R_F2)
    got(R_F2, rf2, n_kv - 1)
    put_rows(tf2, tp, total_of(rf2, range(n_kv)))
    to_all_tp(tf2, T_F2)
    got(T_F2, tf2, n_tp - 1)
    bf = total_of(tf2, range(n_tp))

    stb[kv] = flat(lane_sum(bf * bf))
    to_all_kv(stb, K_STAT)
    got(K_STAT, stb, n_kv - 1)
    line = functools.reduce(lambda a, k: a + stb[k], range(1, n_kv), stb[0])
    scale = lax.rsqrt(upright(line) / width + EPS)
    final = (mid[kv] + 0.5 * (bf * scale * gains[5:6, pl.ds(col, LANES)])).astype(BF16)
    out_ref[...] = nt(place, final)[:, 0:seqs].astype(BF16)

    for stage, buf, n in (
        (T_TOK, ttok, n_tp - 1), (T_F2, tf2, n_tp - 1), (K_TOK, xb, n_kv - 1), (R_F1, pf, n_kv - 1), (P_F1, pb, n_plane - 1),
        (K_QA, qa, nz - 1), (K_QB, qb, nz - 1), (X_Q, wqf, NX - 1), (Z_ST, zst, nz - 1), (K_B, bb, n_kv - NX), (R_ATT, ro, n_kv - 1),
        (R_LSE, rl, n_kv - 1), (P_MIX, rm, n_plane - 1), (K_MIX, mb, n_kv - 1), (R_F2, pf2, n_kv - 1), (K_STAT, stb, n_kv - 1),
    ):
        gone(stage, buf, n)
    wait(ssem.at[X_W], wx.at[:, pl.ds(0, NX - 1)])
    wait(ssem.at[X_WO], wo2.at[pl.ds(0, NX - 1)])

    @pl.when(owns)
    def _():
        gone(Z_OWNL, rl, nz - 1)
        gone(Z_OWN, ro, nz - 1)

    @pl.when(jnp.logical_not(owns))
    def _():
        wait(ssem.at[O_A], oa.at[:, pl.ds(0, seqs)])
        wait(ssem.at[O_B], ob.at[:, pl.ds(0, seqs)])


def solution(mesh):
    n_kv, n_tp = mesh.shape["kv"], mesh.shape["tp"]
    axes = ("kv", "tp")

    def body(tokens, gains, g1, l1, d1, wq, wk, wv, wf, wo, g2, l2, d2, ck, cv, cd):
        seqs, own = tokens.shape
        width = own * n_kv * n_tp
        heads = cd.shape[1]
        groups = heads * HD // LANES
        nz, n_plane = n_kv // NX, NX * n_tp
        arrays = (tokens.T, gains, wq, wk, wv, wf.T, g1.T, l1.T, d1, ck, cd, cv, wo, g2.T, l2.T, d2)
        arrays = tuple(pltpu.with_memory_space_constraint(a, pltpu.HBM) for a in arrays)
        vm = pltpu.VMEM

        def blocks(*n):
            return vm((*n, TILE, LANES), BF16)

        scratch = [vm(a.shape, a.dtype) for i, a in enumerate(arrays) if i != 2] + [
            vm((seqs, heads * HD, cd.shape[2]), BF16),
            blocks(n_tp),
            blocks(n_kv),
            vm((NX, LANES, groups * LANES), BF16),
            vm((2, NX, LANES, LANES), BF16),
            vm((NX, LANES, LANES), BF16),
            blocks(n_kv),
            blocks(n_kv),
            blocks(n_plane),
            blocks(n_kv),
            blocks(nz, groups),
            blocks(nz, groups),
            blocks(3),
            blocks(3),
            blocks(nz, 3),
            blocks(nz, 3),
            vm((nz, 3, LANES), F32),
            vm((groups, ROWS, LANES), F32),
            vm((seqs, heads, cd.shape[2]), F32),
            vm((seqs, heads, cd.shape[2]), BF16),
            vm((seqs, heads, LANES), F32),
            vm((seqs * heads, heads * HD), F32),
            blocks(groups),
            vm((groups, 2, LANES), F32),
            blocks(n_kv + 1),
            vm((n_kv + 1, 2, LANES), F32),
            vm((LANES, LANES), F32),
            vm((n_kv + 1, ROWS, LANES), F32),
            blocks(NX),
            blocks(n_plane),
            blocks(n_kv),
            vm((n_kv, ROWS, LANES), F32),
            blocks(n_kv),
            blocks(n_kv),
            blocks(n_tp),
            vm((n_kv, 1, LANES), F32),
            pltpu.SemaphoreType.DMA((len(arrays),)),
            pltpu.SemaphoreType.DMA((STAGES,)),
            pltpu.SemaphoreType.DMA((STAGES,)),
            pltpu.SemaphoreType.REGULAR((3,)),
        ]
        out = pl.pallas_call(
            functools.partial(kernel, n_kv, n_tp, seqs, width),
            out_shape=jax.ShapeDtypeStruct((own, seqs), BF16),
            in_specs=[pl.BlockSpec(memory_space=pl.ANY)] * len(arrays),
            out_specs=pl.BlockSpec(memory_space=pltpu.VMEM),
            scratch_shapes=scratch,
            compiler_params=pltpu.CompilerParams(
                collective_id=0, has_side_effects=True, vmem_limit_bytes=36 * 1024 * 1024
            ),
            name="layer",
        )(*arrays)
        return out.T

    placed = (
        P(None, axes), P(), P(None, axes), P(None, axes), P(axes, None), P("kv", "tp"), P("kv", "tp"), P("kv", "tp"),
        P(None, "tp"), P("tp", "kv"), P(None, axes), P(None, axes), P(axes, None), P(None, "kv", "tp"),
        P(None, "kv", "tp"), P(None, "tp", "kv"),
    )
    return jax.shard_map(body, mesh=mesh, in_specs=placed, out_specs=P(None, axes), check_vma=False)
```

```python
import functools

import jax
import jax.numpy as jnp
from jax import lax
from jax.experimental import pallas as pl
from jax.experimental.pallas import tpu as pltpu
from jax.sharding import PartitionSpec as P

MESH = pl.DeviceIdType.MESH
F32, BF16 = jnp.float32, jnp.bfloat16
EPS = 1e-06
HD = 64
LANES = 128
ROWS = 24
TILE = 32
NX = 4
STAGES = 22
(T_TOK, K_TOK, X_Q, X_W, X_WO, R_F1, P_F1, K_QA, K_QB, O_A, O_B, Z_ST, Z_OWN, Z_OWNL, K_B, R_ATT, R_LSE, P_MIX, K_MIX,
 R_F2, T_F2, K_STAT) = range(STAGES)


def nt(a, b):
    return lax.dot_general(a, b, (((1,), (1,)), ((), ())), preferred_element_type=F32)


def nn(a, b):
    return jnp.dot(a, b, preferred_element_type=F32)


def lane_sum(v):
    return jnp.sum(v, axis=-1, keepdims=True)


def rows_of(ref, k):
    return ref[k, 0:ROWS, :].astype(F32)


def put_rows(ref, k, v):
    ref[k, 0:ROWS, :] = v.astype(BF16)


def total_of(buf, slots):
    slots = list(slots)
    return functools.reduce(lambda a, k: a + rows_of(buf, k), slots[1:], rows_of(buf, slots[0]))


def padded(v):
    return jnp.concatenate([v, jnp.zeros((ROWS - v.shape[0], v.shape[1]), v.dtype)], axis=0)


def silu(v):
    return v / (1.0 + jnp.exp(-v))


def kernel(
    n_kv, n_tp, seqs, width,
    tok_h, gains_h, wq_h, wk_h, wv_h, wf_h, g1_h, l1_h, d1_h, ck_h, cd_h, cv_h, wo_h, g2_h, l2_h, d2_h,
    out_ref,
    tok, gains, wk, wv, wf, g1, l1, d1, ck, cd, cv, wo, g2, l2, d2,
    ckt, ttok, xb, wqf, wx, wo2, pf, rf, pb, bb, qa, qb, oa, ob, roa, rob, zst, qf, sc, wt, si, om, so, ls, ro, rl, wsq, wexp,
    sm, rm, mb, mid, pf2, rf2, tf2, stb,
    load_sem, ssem, rsem, hello,
):
    kv, tp = lax.axis_index("kv"), lax.axis_index("tp")
    nz = n_kv // NX
    zz, xx = kv // NX, kv % NX
    n_plane = NX * n_tp
    me = xx * n_tp + tp
    heads = cd.shape[1]
    groups = heads * HD // LANES
    zwide = NX * LANES
    zcol = pl.multiple_of(zz * zwide, LANES)
    xcol = pl.multiple_of(xx * LANES, LANES)
    col = pl.multiple_of(kv * LANES, LANES)

    loads = [
        pltpu.make_async_copy(h, v, load_sem.at[i])
        for i, (h, v) in enumerate(
            [(tok_h, tok), (gains_h, gains), (wq_h, wqf.at[xx]), (wk_h, wk), (wv_h, wv), (wf_h, wf), (g1_h, g1), (l1_h, l1),
             (d1_h, d1), (ck_h, ck), (cd_h, cd), (cv_h, cv), (wo_h, wo), (g2_h, g2), (l2_h, l2), (d2_h, d2)]
        )
    ]
    for copy in loads:
        copy.start()

    def ordered(i, n):
        return (n // 2 + ((i + 1) // 2) * (1 - 2 * (i % 2)) + n) % n

    def shift(i, d, n):
        return lax.rem(i + d, n)

    def kv_at(dz, dx):
        return shift(zz, dz % nz, nz) * NX + shift(xx, dx, NX)

    x_of = [shift(xx, ordered(i, NX), NX) for i in range(NX)]

    def at(x):
        return zz * NX + x

    def each_kv(visit, same_z=True):
        @pl.loop(0, nz - 1)
        def _(i):
            first = shift(zz, ordered(i, nz), nz) * NX
            for x in x_of:
                visit(first + x, x)

        if same_z:
            for x in x_of[:-1]:
                visit(at(x), x)

    def each_plane(visit):
        @pl.loop(0, n_tp - 1)
        def _(i):
            t = shift(tp, ordered(i, n_tp), n_tp)
            for x in x_of:
                visit(x, t)

        for x in x_of[:-1]:
            visit(x, tp)

    z_own = (2 * xx + tp) % nz
    owns = zz == z_own

    def send(src, dst, stage, **where):
        pltpu.make_async_remote_copy(
            src_ref=src, dst_ref=dst, send_sem=ssem.at[stage], recv_sem=rsem.at[stage],
            device_id=where, device_id_type=MESH,
        ).start()

    def wait(sem, ref):
        pltpu.make_async_copy(ref, ref, sem).wait()

    def part(buf, slot):
        if buf.shape[-2] != TILE:
            return buf.at[slot]
        if len(buf.shape) == 4:
            return buf.at[slot, :, pl.ds(0, seqs)]
        return buf.at[slot, pl.ds(0, seqs)]

    def got(stage, buf, n):
        wait(rsem.at[stage], part(buf, pl.ds(0, n)))

    def gone(stage, buf, n):
        wait(ssem.at[stage], part(buf, pl.ds(0, n)))

    def to_all_kv(buf, stage, same_z=True):
        each_kv(lambda k, x: send(part(buf, kv), part(buf, kv), stage, kv=k), same_z)

    def to_all_tp(buf, stage):
        @pl.loop(0, n_tp - 1)
        def _(i):
            send(part(buf, tp), part(buf, tp), stage, tp=shift(tp, ordered(i, n_tp), n_tp))

    def to_all_z(buf, slot, stage):
        @pl.loop(0, nz - 1)
        def _(i):
            send(part(buf, slot), part(buf, slot), stage, kv=shift(zz, ordered(i, nz), nz) * NX + xx)

    def to_kv_blocks(src, dst, stage):
        each_kv(lambda k, x: send(part(src, k), part(dst, kv), stage, kv=k))
        dst[kv] = src[kv]

    barrier = pltpu.get_barrier_semaphore()
    for i in range(n_tp - 1):
        pl.semaphore_signal(barrier, inc=1, device_id={"tp": shift(tp, i + 1, n_tp)}, device_id_type=MESH)
    for dz, dx in [(0, d) for d in range(1, NX)] + [(1, 0), (-1, 0)]:
        pl.semaphore_signal(barrier, inc=1, device_id={"kv": kv_at(dz, dx)}, device_id_type=MESH)

    loads[0].wait()
    own_w = tok.shape[0]
    lane = lax.broadcasted_iota(jnp.int32, (own_w, LANES), 1)
    row = lax.broadcasted_iota(jnp.int32, (own_w, LANES), 0)
    place = jnp.where(lane == row + own_w * tp, 1.0, 0.0).astype(BF16)
    mine = lax.dot_general(tok[...], place, (((0,), (0,)), ((), ())), preferred_element_type=F32)
    put_rows(ttok, tp, padded(mine))

    pl.semaphore_wait(barrier, n_tp - 1 + NX - 1 + 2)

    def hear(n, step):
        for dz in (step, -step):
            pl.semaphore_signal(hello.at[n], inc=1, device_id={"kv": kv_at(dz, 0)}, device_id_type=MESH)
        if n != 1:
            pl.semaphore_wait(hello.at[n], 2)

    to_all_tp(ttok, T_TOK)
    hear(0, 1)
    hear(1, 2)
    for i in range(3, 5):
        loads[i].wait()
    for d in range(1, NX):
        j = shift(xx, d, NX)
        for m, w in enumerate((wk, wv)):
            send(w.at[:, pl.ds(pl.multiple_of(j * LANES, LANES), LANES)], wx.at[m, xx], X_W, kv=at(j))
    pl.semaphore_wait(hello.at[1], 2)
    hear(2, 1)
    for m, w in enumerate((wk, wv)):
        wx[m, xx] = w[:, pl.ds(xcol, LANES)]
    got(T_TOK, ttok, n_tp - 1)
    put_rows(xb, kv, total_of(ttok, range(n_tp)))
    to_all_kv(xb, K_TOK)
    loads[2].wait()
    for x in x_of[:-1]:
        send(wqf.at[xx], wqf.at[xx], X_Q, kv=at(x))

    def gain(i, k):
        return gains[i : i + 1, k * LANES : (k + 1) * LANES]

    def zgain(i):
        return gains[i : i + 1, pl.ds(zcol, zwide)]

    def products(block, gain_row, gate_w, lift_w):
        squares, gate, lift = [jnp.zeros((ROWS, n), F32) for n in (LANES, gate_w.shape[0], lift_w.shape[0])]
        for c in range(0, n_kv, 4):
            xs = []
            for k in range(c, c + 4):
                v = block(k)
                squares = squares + v * v
                xs.append((v * gain(gain_row, k)).astype(BF16))
            x = jnp.concatenate(xs, axis=1)
            here = slice(c * LANES, (c + 4) * LANES)
            gate = gate + nt(x, gate_w[:, here])
            lift = lift + nt(x, lift_w[:, here])
        return lane_sum(squares), gate, lift

    def feed_forward(scale, gate, lift, down_w, part_out):
        act = (silu(gate * scale) * (lift * scale)).astype(BF16)
        for c in range(0, n_kv, 4):
            some = nn(act, down_w[:, c * LANES : (c + 4) * LANES])
            for j in range(4):
                put_rows(part_out, c + j, some[:, j * LANES : (j + 1) * LANES])

    lane_r = lax.broadcasted_iota(jnp.int32, (ROWS, LANES), 1)
    low = lane_r < HD
    eye = lax.broadcasted_iota(jnp.int32, (ROWS, LANES), 0) == lane_r

    def flat(column):
        return jnp.sum(jnp.where(eye, column, 0.0), axis=0, keepdims=True)

    def upright(line):
        return lane_sum(jnp.where(eye, jnp.broadcast_to(line, (ROWS, LANES)), 0.0))

    loads[1].wait()
    got(K_TOK, xb, n_kv - 1)
    for i in range(6, 9):
        loads[i].wait()
    s_tt, gate, lift = products(lambda k: rows_of(xb, k), 0, g1, l1)
    feed_forward(lax.rsqrt(s_tt / width + EPS), gate, lift, d1, pf)
    to_kv_blocks(pf, rf, R_F1)

    loads[9].wait()

    @pl.loop(0, seqs)
    def _(b):
        ckt[b] = ck[b].T

    loads[5].wait()
    wait(rsem.at[X_W], wx.at[:, pl.ds(0, NX - 1)])
    got(X_Q, wqf, NX - 1)
    tz = jnp.concatenate([rows_of(xb, at(x)) for x in range(NX)], axis=1)
    lane_f = lax.broadcasted_iota(jnp.int32, (ROWS, heads), 1)

    def query_part(x, q_out):
        q = nn(x, wqf[...].reshape(zwide, groups * LANES))
        for j in range(groups):
            q_out[zz, j, 0:ROWS, :] = q[:, j * LANES : (j + 1) * LANES].astype(BF16)

    def other_parts(x, o_out):
        for m in range(2):
            put_rows(o_out, m, nn(x, wx[m].reshape(zwide, LANES)))
        f = nt(x, wf[:, pl.ds(zcol, zwide)])
        f0, f1 = [lane_sum(jnp.where(lane_f == 2 * xx + g, f, 0.0)) for g in range(2)]
        put_rows(o_out, 2, jnp.where(low, f0, f1))

    def to_owner(src, dst, stage):
        whole = src.at[:, pl.ds(0, seqs)]

        @pl.when(jnp.logical_not(owns))
        def _():
            send(whole, dst.at[zz, :, pl.ds(0, seqs)], stage, kv=z_own * NX + xx)

        @pl.when(owns)
        def _():
            dst[zz] = src[...]

    shared = (tz * zgain(2)).astype(BF16)
    query_part(shared, qa)
    other_parts(shared, oa)

    got(R_F1, rf, n_kv - 1)
    put_rows(pb, me, total_of(rf, range(n_kv)))

    def to_plane(src, dst, stage, pick):
        each_plane(lambda x, t: send(part(src, pick(x)), part(dst, me), stage, kv=at(x), tp=t))

    to_plane(pb, pb, P_F1, lambda x: me)
    to_all_z(qa, zz, K_QA)
    to_owner(oa, roa, O_A)

    got(P_F1, pb, n_plane - 1)
    for x in range(NX):
        put_rows(bb, at(x), total_of(pb, range(x * n_tp, (x + 1) * n_tp)))
    bz = jnp.concatenate([rows_of(bb, at(x)) for x in range(NX)], axis=1)
    u = bz * zgain(1)
    shared = (u * zgain(2)).astype(BF16)
    query_part(shared, qb)
    for n, stat in enumerate((bz * bz, tz * u, u * u)):
        zst[zz, n : n + 1, :] = flat(lane_sum(stat))
    to_all_z(zst, zz, Z_ST)
    to_all_z(qb, zz, K_QB)
    other_parts(shared, ob)
    to_owner(ob, rob, O_B)

    got(K_QA, qa, nz - 1)
    got(Z_ST, zst, nz - 1)
    stats = functools.reduce(lambda a, z: a + zst[z], range(1, nz), zst[0])
    s_bb, s_tu, s_uu = [upright(stats[n : n + 1]) for n in range(3)]
    r1 = lax.rsqrt(s_bb / width + EPS)
    half = 0.5 * r1
    scale_mid = lax.rsqrt(jnp.maximum(s_tt + r1 * s_tu + half * half * s_uu, 0.0) / width + EPS)

    def z_sum(buf, j):
        return functools.reduce(lambda a, b: a + b, [buf[z, j, 0:ROWS, :].astype(F32) for z in range(nz)])

    from_tokens = [z_sum(qa, j) for j in range(groups)]
    got(K_QB, qb, nz - 1)
    for j in range(groups):
        qf[j] = (scale_mid * (from_tokens[j] + half * z_sum(qb, j))).astype(BF16).astype(F32)

    loads[12].wait()
    for d in range(1, NX):
        j = shift(xx, d, NX)
        send(wo.at[pl.ds(pl.multiple_of(j * LANES, LANES), LANES), :], wo2.at[xx], X_WO, kv=at(j))
    wo2[xx] = wo[pl.ds(xcol, LANES), :]
    for i in range(10, 12):
        loads[i].wait()
    head_i = lax.broadcasted_iota(jnp.int32, (heads, LANES), 0)
    lane_h = lax.broadcasted_iota(jnp.int32, (heads, LANES), 1)
    masks = [head_i == 2 * j + lane_h // HD for j in range(groups)]
    for b in range(seqs):
        rows = [jnp.where(masks[j], jnp.broadcast_to(qf[j, b : b + 1, :], (heads, LANES)), 0.0) for j in range(groups)]
        query = jnp.concatenate(rows, axis=1).astype(BF16)
        sc[b] = nn(query, ckt[b]) * (HD**-0.5) + cd[b]

    score = sc[...]
    peak = jnp.max(score, axis=2, keepdims=True)
    raised = jnp.exp(score - peak)
    total = jnp.sum(raised, axis=2, keepdims=True)
    wt[...] = raised.astype(BF16)
    si[...] = jnp.broadcast_to(1.0 / total, (seqs, heads, LANES))
    level = jnp.broadcast_to(peak + jnp.log(total), (seqs, heads, LANES))
    turn = lax.broadcasted_iota(jnp.int32, (seqs, heads, LANES), 0) == lax.broadcasted_iota(
        jnp.int32, (seqs, heads, LANES), 2
    )
    lines = jnp.sum(jnp.where(turn, level, 0.0), axis=0)
    for j in range(groups):
        ls[j] = lines[2 * j : 2 * j + 2]

    for i in range(n_kv - 1):
        first, x = shift(zz, ordered(i // NX, nz), nz) * NX, x_of[i % NX]
        send(ls.at[x], rl.at[kv], R_LSE, kv=first + x)
    rl[kv] = ls[xx]

    for b in range(seqs):
        o = nn(wt[b], cv[b])
        share = si[b]
        for j in range(groups):
            om[b * heads : (b + 1) * heads, j * LANES : (j + 1) * LANES] = jnp.where(
                masks[j], o[:, j * LANES : (j + 1) * LANES] * share, 0.0
            )

    pick = lax.broadcasted_iota(jnp.int32, (ROWS, seqs * heads), 1) // heads
    pick = jnp.where(pick == lax.broadcasted_iota(jnp.int32, (ROWS, seqs * heads), 0), 1.0, 0.0).astype(BF16)
    outs = nn(pick, om[...].astype(BF16))
    for j in range(groups):
        put_rows(so, j, outs[:, j * LANES : (j + 1) * LANES])

    each_kv(lambda k, x: send(part(so, x), part(ro, kv), R_ATT, kv=k))
    ro[kv] = so[xx]

    @pl.when(owns)
    def _():
        got(O_A, roa, nz - 1)
        got(O_B, rob, nz - 1)

        def finished(n):
            a = functools.reduce(lambda t, z: t + roa[z, n, 0:ROWS, :].astype(F32), range(1, nz), roa[0, n, 0:ROWS, :].astype(F32))
            b = functools.reduce(lambda t, z: t + rob[z, n, 0:ROWS, :].astype(F32), range(1, nz), rob[0, n, 0:ROWS, :].astype(F32))
            return scale_mid * (a + half * b)

        k, v, f = [finished(n) for n in range(3)]
        qk = qf[xx] * k.astype(BF16).astype(F32)
        forget = jnp.minimum(f, 0.0) - jnp.log(1.0 + jnp.exp(-jnp.abs(f)))
        own0 = lane_sum(jnp.where(low, qk, 0.0)) * (HD**-0.5) - forget[:, 0:1]
        own1 = lane_sum(jnp.where(low, 0.0, qk)) * (HD**-0.5) - forget[:, HD : HD + 1]
        put_rows(ro, n_kv, v)
        rl[n_kv, 0:1, :] = flat(own0)
        rl[n_kv, 1:2, :] = flat(own1)
        to_all_z(rl, n_kv, Z_OWNL)
        to_all_z(ro, n_kv, Z_OWN)

    @pl.when(jnp.logical_not(owns))
    def _():
        wait(rsem.at[Z_OWNL], rl.at[n_kv])

    got(R_LSE, rl, n_kv - 1)
    n_src = n_kv + 1
    top = functools.reduce(jnp.maximum, [rl[s] for s in range(n_src)])
    raised = [jnp.exp(rl[s] - top) for s in range(n_src)]
    norm = 1.0 / functools.reduce(lambda a, b: a + b, raised)
    for s in range(n_src):
        wsq[2 * s : 2 * s + 2, :] = raised[s] * norm
    weights = wsq[...].T[0:ROWS]
    for s in range(n_src):
        wexp[s] = jnp.where(low, weights[:, 2 * s : 2 * s + 1], weights[:, 2 * s + 1 : 2 * s + 2])

    @pl.when(jnp.logical_not(owns))
    def _():
        wait(rsem.at[Z_OWN], part(ro, n_kv))

    got(R_ATT, ro, n_kv - 1)
    joined = jnp.zeros((ROWS, LANES), F32)
    for s in range(n_src):
        joined = joined + wexp[s] * rows_of(ro, s)
    attended = joined.astype(BF16)
    wait(rsem.at[X_WO], wo2.at[pl.ds(0, NX - 1)])
    for x in range(NX):
        put_rows(sm, x, nn(attended, wo2[x]))

    to_plane(sm, rm, P_MIX, lambda x: x)
    rm[me] = sm[xx]
    to_all_kv(bb, K_B, False)
    got(P_MIX, rm, n_plane - 1)
    put_rows(mb, kv, total_of(rm, range(n_plane)))

    to_all_kv(mb, K_MIX)
    for i in range(13, 16):
        loads[i].wait()

    got(K_B, bb, n_kv - NX)
    for k in range(n_kv):
        mid[k] = rows_of(xb, k) + rows_of(bb, k) * half * gain(1, k)

    got(K_MIX, mb, n_kv - 1)

    squares = jnp.zeros((ROWS, LANES), F32)
    for k in range(n_kv):
        v = rows_of(mb, k)
        squares = squares + v * v
    scale = lax.rsqrt(lane_sum(squares) / width + EPS)

    def after(k):
        mid[k] = mid[k] + rows_of(mb, k) * scale * gain(3, k)
        return mid[k]

    s_aa, gate, lift = products(after, 4, g2, l2)
    feed_forward(lax.rsqrt(s_aa / width + EPS), gate, lift, d2, pf2)
    to_kv_blocks(pf2, rf2, R_F2)
    got(R_F2, rf2, n_kv - 1)
    put_rows(tf2, tp, total_of(rf2, range(n_kv)))
    to_all_tp(tf2, T_F2)
    got(T_F2, tf2, n_tp - 1)
    bf = total_of(tf2, range(n_tp))

    stb[kv] = flat(lane_sum(bf * bf))
    to_all_kv(stb, K_STAT)
    got(K_STAT, stb, n_kv - 1)
    line = functools.reduce(lambda a, k: a + stb[k], range(1, n_kv), stb[0])
    scale = lax.rsqrt(upright(line) / width + EPS)
    final = (mid[kv] + 0.5 * (bf * scale * gains[5:6, pl.ds(col, LANES)])).astype(BF16)
    out_ref[...] = nt(place, final)[:, 0:seqs].astype(BF16)

    for stage, buf, n in (
        (T_TOK, ttok, n_tp - 1), (T_F2, tf2, n_tp - 1), (K_TOK, xb, n_kv - 1), (R_F1, pf, n_kv - 1), (P_F1, pb, n_plane - 1),
        (K_QA, qa, nz - 1), (K_QB, qb, nz - 1), (X_Q, wqf, NX - 1), (Z_ST, zst, nz - 1), (K_B, bb, n_kv - NX), (R_ATT, ro, n_kv - 1),
        (R_LSE, rl, n_kv - 1), (P_MIX, rm, n_plane - 1), (K_MIX, mb, n_kv - 1), (R_F2, pf2, n_kv - 1), (K_STAT, stb, n_kv - 1),
    ):
        gone(stage, buf, n)
    wait(ssem.at[X_W], wx.at[:, pl.ds(0, NX - 1)])
    wait(ssem.at[X_WO], wo2.at[pl.ds(0, NX - 1)])

    @pl.when(owns)
    def _():
        gone(Z_OWNL, rl, nz - 1)
        gone(Z_OWN, ro, nz - 1)

    @pl.when(jnp.logical_not(owns))
    def _():
        wait(ssem.at[O_A], oa.at[:, pl.ds(0, seqs)])
        wait(ssem.at[O_B], ob.at[:, pl.ds(0, seqs)])


def solution(mesh):
    n_kv, n_tp = mesh.shape["kv"], mesh.shape["tp"]
    axes = ("kv", "tp")

    def body(tokens, gains, g1, l1, d1, wq, wk, wv, wf, wo, g2, l2, d2, ck, cv, cd):
        seqs, own = tokens.shape
        width = own * n_kv * n_tp
        heads = cd.shape[1]
        groups = heads * HD // LANES
        nz, n_plane = n_kv // NX, NX * n_tp
        arrays = (tokens.T, gains, wq, wk, wv, wf.T, g1.T, l1.T, d1, ck, cd, cv, wo, g2.T, l2.T, d2)
        arrays = tuple(pltpu.with_memory_space_constraint(a, pltpu.HBM) for a in arrays)
        vm = pltpu.VMEM

        def blocks(*n):
            return vm((*n, TILE, LANES), BF16)

        scratch = [vm(a.shape, a.dtype) for i, a in enumerate(arrays) if i != 2] + [
            vm((seqs, heads * HD, cd.shape[2]), BF16),
            blocks(n_tp),
            blocks(n_kv),
            vm((NX, LANES, groups * LANES), BF16),
            vm((2, NX, LANES, LANES), BF16),
            vm((NX, LANES, LANES), BF16),
            blocks(n_kv),
            blocks(n_kv),
            blocks(n_plane),
            blocks(n_kv),
            blocks(nz, groups),
            blocks(nz, groups),
            blocks(3),
            blocks(3),
            blocks(nz, 3),
            blocks(nz, 3),
            vm((nz, 3, LANES), F32),
            vm((groups, ROWS, LANES), F32),
            vm((seqs, heads, cd.shape[2]), F32),
            vm((seqs, heads, cd.shape[2]), BF16),
            vm((seqs, heads, LANES), F32),
            vm((seqs * heads, heads * HD), F32),
            blocks(groups),
            vm((groups, 2, LANES), F32),
            blocks(n_kv + 1),
            vm((n_kv + 1, 2, LANES), F32),
            vm((LANES, LANES), F32),
            vm((n_kv + 1, ROWS, LANES), F32),
            blocks(NX),
            blocks(n_plane),
            blocks(n_kv),
            vm((n_kv, ROWS, LANES), F32),
            blocks(n_kv),
            blocks(n_kv),
            blocks(n_tp),
            vm((n_kv, 1, LANES), F32),
            pltpu.SemaphoreType.DMA((len(arrays),)),
            pltpu.SemaphoreType.DMA((STAGES,)),
            pltpu.SemaphoreType.DMA((STAGES,)),
            pltpu.SemaphoreType.REGULAR((3,)),
        ]
        out = pl.pallas_call(
            functools.partial(kernel, n_kv, n_tp, seqs, width),
            out_shape=jax.ShapeDtypeStruct((own, seqs), BF16),
            in_specs=[pl.BlockSpec(memory_space=pl.ANY)] * len(arrays),
            out_specs=pl.BlockSpec(memory_space=pltpu.VMEM),
            scratch_shapes=scratch,
            compiler_params=pltpu.CompilerParams(
                collective_id=0, has_side_effects=True, vmem_limit_bytes=36 * 1024 * 1024
            ),
            name="layer",
        )(*arrays)
        return out.T

    placed = (
        P(None, axes), P(), P(None, axes), P(None, axes), P(axes, None), P("kv", "tp"), P("kv", "tp"), P("kv", "tp"),
        P(None, "tp"), P("tp", "kv"), P(None, axes), P(None, axes), P(axes, None), P(None, "kv", "tp"),
        P(None, "kv", "tp"), P(None, "tp", "kv"),
    )
    return jax.shard_map(body, mesh=mesh, in_specs=placed, out_specs=P(None, axes), check_vma=False)
```
